32 devices in a mesh: kv: 8 (over z, x), tp: 4 (over y, core).
Axes of the slice: x: 2, y: 2, z: 4, core: 2. Of those that a mesh axis runs over, the one named last changes fastest.
Arguments:
- inputs: bfloat16 [4, 2048, 2048], P(None, 'kv'), may hold values from -40 to 40
- query_weight: bfloat16 [2048, 2048], P(None, 'tp'), may hold values from -0.125 to 0.125
- key_weight: bfloat16 [2048, 1024], P(None, 'tp'), may hold values from -0.125 to 0.125
- value_weight: bfloat16 [2048, 1024], P(None, 'tp'), may hold values from -0.125 to 0.125
- out_weight: bfloat16 [2048, 2048], P('tp'), may hold values from -1 to 1
- chosen: int32 [4, 32, 32], P(None, 'kv'), may hold values from 0 to 31, as said below
- lengths: int32 [4], replicated, may hold values from 1 to 2048, 3072 in all
Outputs:
- mixed: bfloat16 [4, 2048, 2048], P(None, 'kv', 'tp')
The draws below stay inside these ranges and needn't reach their ends.
Inputs may be any that keep to these rules, and one draw needn't show every extreme that they name: chosen[b, q, 0] = q; every entry names a block of the same sequence at or before q; entries may repeat. Over the query blocks of positions k * 256 to (k+1) * 256 - 1 of all sequences, the named blocks that lie in another span of 256 positions number at most 3 distinct blocks for each other span, and 3 is reached.
All inputs are finite; a program needn't handle non-finite values.
Results may differ from the reference program's by a relative error of at most 0.014.
The reference program's roundings to bfloat16 on the way count: a program that leaves them out, or rounds other values in their place, can miss the bound.
Values may be sent and summed in bfloat16 or wider, within the bound.
A program may use at most 128 MiB of HBM per device.

```python
import math
import jax
import jax.numpy as jnp
import numpy as np
from jax import lax

D = 2048
HEADS = 16
KV_HEADS = 8
HD = 128
KB = 64
TOPK = 32
CAP = 3
BATCH = 4
SEQ_DEV = 256
SEQ = 2048
NB = 32
N_TP = 4


def draw_inputs(key, part):
    key_base = jax.random.fold_in(jax.random.fold_in(key, 3), 0)
    entries = jax.random.normal(key_base, (BATCH, SEQ, D), jnp.float32)
    return jnp.clip(entries, -40.0, 40.0).astype(jnp.bfloat16)


def draw_chosen(key, part):
    per_dev = SEQ_DEV // KB
    ndevices = NB // per_dev
    owned = BATCH * per_dev
    key_count, key_rank, key_order = jax.random.split(jax.random.fold_in(key, 7), 3)
    receiver = jnp.arange(ndevices, dtype=jnp.int32)[:, None]
    sender = jnp.arange(ndevices, dtype=jnp.int32)[None, :]
    counts = jax.random.randint(key_count, (ndevices, ndevices), 1, CAP + 1)
    counts = jnp.where(sender == receiver - 1, CAP, counts)
    counts = jnp.where(sender < receiver, counts, 0)
    local_ids = jnp.arange(owned, dtype=jnp.int32)
    noise = jax.random.randint(key_rank, (ndevices, ndevices, owned), 0, 1 << 20) * owned + local_ids
    ranks = jnp.argsort(jnp.argsort(noise, axis=-1), axis=-1)
    picked = ranks < counts[:, :, None]
    order_noise = jax.random.randint(key_order, (ndevices, ndevices), 0, 1 << 20) * ndevices + sender
    priority = jnp.argsort(jnp.argsort(order_noise, axis=-1), axis=-1) + 2
    priority = jnp.where(sender == receiver - ndevices // 2, 1, priority)
    priority = jnp.where(sender == receiver - 1, 0, priority)
    seq_of = local_ids // per_dev
    global_block = sender[:, :, None] * per_dev + (local_ids % per_dev)[None, None, :]
    big_score = (ndevices + 4) * owned
    seq_range = jnp.arange(BATCH, dtype=jnp.int32)
    in_seq = picked[:, None, :, :] & (seq_of[None, None, None, :] == seq_range[None, :, None, None])
    scored = jnp.where(in_seq, priority[:, None, :, None] * owned + local_ids[None, None, None, :], big_score)
    scored = scored.reshape(ndevices, BATCH, ndevices * owned)
    sorted_idx = jnp.argsort(scored, axis=-1)
    pool_size = jnp.sum(in_seq.reshape(ndevices, BATCH, ndevices * owned).astype(jnp.int32), axis=-1)
    pool_blocks = jnp.take_along_axis(jnp.broadcast_to(global_block.reshape(1, 1, ndevices * owned), (ndevices, BATCH, ndevices * owned)), sorted_idx, axis=-1)
    local_row = jnp.arange(per_dev, dtype=jnp.int32)[:, None]
    slot_col = jnp.arange(TOPK, dtype=jnp.int32)[None, :]
    base_count = local_row * (TOPK - 1) - local_row * (local_row - 1) // 2
    counter = base_count + slot_col - 1 - local_row
    safe_size = jnp.maximum(pool_size, 1)
    pool_pick = jnp.take_along_axis(pool_blocks, counter.reshape(1, 1, -1) % safe_size[:, :, None], axis=-1)
    pool_pick = pool_pick.reshape(ndevices, BATCH, per_dev, TOPK)
    own_block = jnp.arange(ndevices, dtype=jnp.int32)[:, None, None, None] * per_dev + local_row[None, None, :, :] + 0 * slot_col[None, None, :, :]
    earlier = own_block - local_row[None, None, :, :] + slot_col[None, None, :, :] - 1
    result = jnp.where(pool_size[:, :, None, None] > 0, pool_pick, own_block)
    result = jnp.where((slot_col >= 1) & (slot_col <= local_row), earlier, result)
    result = jnp.where(slot_col == 0, own_block, result)
    return jnp.transpose(result, (1, 0, 2, 3)).reshape(BATCH, NB, TOPK).astype(jnp.int32)


def level_of(stream_key, dims, cuts, smallest, largest):
    level = 1.0
    for dim, parts in cuts:
        steps = jax.random.uniform(jax.random.fold_in(jax.random.fold_in(stream_key, 6), dim), (parts,), jnp.float32, smallest / len(cuts), largest / len(cuts))
        level = level * jnp.repeat(jnp.exp(steps), dims[dim] // parts).reshape((-1,) + (1,) * (len(dims) - 1 - dim))
    return level


def profile(count, total, reach, lean):
    portions = [(1 << 20) // math.isqrt(grade ** lean) + 1 for grade in range(2, count + 1)]
    surplus, given = total - reach - (count - 1), [1] * (count - 1)
    while surplus > 0:
        candidates = [i for i in range(count - 1) if given[i] < reach]
        mass, budget = sum([portions[i] for i in candidates]), surplus
        for i in candidates:
            addition = min(reach - given[i], max(1, budget * portions[i] // mass), surplus)
            given[i] = given[i] + addition
            surplus = surplus - addition
    return np.array([reach] + given)


def uneven(key, amount, total, bound, slope):
    if amount == 2:
        one = jax.random.randint(key, (), max(1, total - bound), min(bound, total - 1) + 1)
        return jnp.stack([one, total - one])
    tallies = jnp.asarray(profile(amount, total, bound, slope), jnp.int32)
    pairs = (amount - 1) // 2
    source_of, taker = tallies[1:1 + 2 * pairs:2], tallies[2:2 + 2 * pairs:2]
    margin = jnp.minimum(source_of - 1, bound - taker)
    moved = jax.random.randint(jax.random.fold_in(key, 1), (pairs,), 0, 1 << 20) % (margin + 1)
    tallies = tallies.at[1:1 + 2 * pairs:2].set(source_of - moved).at[2:2 + 2 * pairs:2].set(taker + moved)
    return tallies[jax.random.permutation(jax.random.fold_in(key, 2), amount)]


def gaussian(stream_key, extent, spread, bound, pieces=(), kind=jnp.bfloat16):
    array = jax.random.normal(stream_key, extent, jnp.float32) * spread
    if len(pieces) > 0:
        array = level_of(stream_key, extent, pieces, -0.22, 0.18) * array
    return jnp.clip(array, min=-bound, max=bound).astype(kind)


def setup_inputs(seed: int = 0) -> dict:
    seeds = jax.random.split(jax.random.key(seed), 8)
    return {
        "inputs": draw_inputs(jax.random.fold_in(seeds[7], 71), 0),
        "query_weight": gaussian(seeds[1], (D, HEADS * HD), D ** -0.5, 0.125, ((1, 4),)),
        "key_weight": gaussian(seeds[2], (D, KV_HEADS * HD), D ** -0.5, 0.125, ((1, 4),)),
        "value_weight": gaussian(seeds[3], (D, KV_HEADS * HD), D ** -0.5, 0.125, ((1, 4),)),
        "out_weight": gaussian(seeds[4], (HEADS * HD, D), (HEADS * HD // 64) ** -0.5, 1.0, ((0, 4),)),
        "chosen": draw_chosen(jax.random.fold_in(seeds[7], 71), 0),
        "lengths": uneven(seeds[6], BATCH, SEQ + SEQ // 2, SEQ, 2).astype(jnp.int32),
    }


def unique_slots(chosen_rows):
    order = jnp.arange(TOPK, dtype=jnp.int32)
    repeated = jnp.any((chosen_rows[..., :, None] == chosen_rows[..., None, :]) & (order[:, None] > order[None, :]), axis=-1)
    return jnp.repeat(jnp.logical_not(repeated), KB, axis=-1)


def attend(queries, key_sets, value_sets, key_pos, unique_key, query_pos, live_length):
    scores = jnp.einsum("nqkgd,npkd->nkgqp", queries.astype(jnp.float32), key_sets.astype(jnp.float32)) * (HD ** -0.5)
    allowed = (key_pos[:, None, :] <= query_pos[:, :, None]) & (key_pos[:, None, :] < live_length) & unique_key[:, None, :]
    allowed = allowed | (key_pos[:, None, :] == query_pos[:, :, None])
    scores = jnp.where(allowed[:, None, None], scores, -jnp.inf)
    highest = jnp.max(scores, axis=-1, keepdims=True)
    raised = jnp.exp(scores - highest)
    weights = (raised / jnp.sum(raised, axis=-1, keepdims=True)).astype(jnp.bfloat16)
    combined = jnp.einsum("nkgqp,npkd->nqkgd", weights.astype(jnp.float32), value_sets.astype(jnp.float32))
    living = (query_pos < live_length)[:, :, None, None, None]
    return jnp.where(living, combined, 0.0).astype(jnp.bfloat16)


def reference(inputs, query_weight, key_weight, value_weight, out_weight, chosen, lengths):
    per_group = HEADS // KV_HEADS
    flat_rows = inputs.reshape(BATCH * SEQ, D)
    queries = jnp.dot(flat_rows, query_weight, preferred_element_type=jnp.float32).astype(jnp.bfloat16)
    queries = queries.reshape(BATCH, NB, KB, KV_HEADS, per_group, HD)
    key_rows = jnp.dot(flat_rows, key_weight, preferred_element_type=jnp.float32).astype(jnp.bfloat16)
    key_rows = key_rows.reshape(BATCH, NB, KB, KV_HEADS, HD)
    value_rows = jnp.dot(flat_rows, value_weight, preferred_element_type=jnp.float32).astype(jnp.bfloat16)
    value_rows = value_rows.reshape(BATCH, NB, KB, KV_HEADS, HD)
    offsets = jnp.arange(KB, dtype=jnp.int32)

    def one_block(block_pair):
        seq_index, block_id = block_pair
        names = chosen[seq_index, block_id]
        key_sets = key_rows[seq_index][names].reshape(1, TOPK * KB, KV_HEADS, HD)
        value_sets = value_rows[seq_index][names].reshape(1, TOPK * KB, KV_HEADS, HD)
        key_pos = (names[:, None] * KB + offsets[None, :]).reshape(1, TOPK * KB)
        query_pos = (block_id * KB + offsets)[None, :]
        unique_key = unique_slots(names)[None, :]
        result = attend(queries[seq_index, block_id][None], key_sets, value_sets, key_pos, unique_key, query_pos, lengths[seq_index])
        return result[0]

    seq_ids = jnp.repeat(jnp.arange(BATCH, dtype=jnp.int32), NB)
    block_ids = jnp.tile(jnp.arange(NB, dtype=jnp.int32), BATCH)
    attended = lax.map(one_block, (seq_ids, block_ids)).reshape(BATCH * SEQ, HEADS * HD)
    group_width = HEADS * HD // N_TP
    summed = jnp.zeros((BATCH * SEQ, D), jnp.float32)
    for group_id in range(N_TP):
        partial_value = jnp.dot(attended[:, group_id * group_width:(group_id + 1) * group_width],
                          out_weight[group_id * group_width:(group_id + 1) * group_width],
                          preferred_element_type=jnp.float32).astype(jnp.bfloat16)
        summed = summed + lax.optimization_barrier(partial_value).astype(jnp.float32)
    return summed.astype(jnp.bfloat16).reshape(BATCH, SEQ, D)
```

```python
import functools

import jax
import jax.numpy as jnp
from jax import lax
from jax.experimental import pallas as pl
from jax.experimental.pallas import tpu as pltpu
from jax.sharding import PartitionSpec as P

HD = 128
KB = 64
MASKED = -1e30
PIECES = 2
STEP_ROWS = 128
MESH = pl.DeviceIdType.MESH


def spans(batch_size, devices, positions):
    seq = devices * positions
    total = seq + seq // 2
    longest = [min(seq, (total - (batch_size - 1 - j)) // (j + 1)) for j in range(batch_size)]
    return tuple(-(-length // positions) for length in longest)


def layer_kernel(
    reach, columns, kv_local, per_group, tp,
    length_ref, x_hbm, wq_hbm, wk_hbm, wv_hbm, wo_hbm, chosen_ref, out_ref,
    x_ref, wq_ref, wkv_ref, wo_ref, stage_ref, kv_ref, q_ref,
    top_ref, total_ref, acc_ref, att_ref,
    pair_out, pair_in, far_out, far_in, near, mixed_ref,
    load_sem, z_sent, x_sent, got, pair_sent, pair_got, far_sent, far_got,
):
    batch_size, positions, _ = x_ref.shape
    slots, devices = kv_ref.shape[:2]
    rows_z = devices // columns
    per_dev = positions // KB
    half = kv_local * HD
    rows = per_group * positions
    width = out_ref.shape[-1]
    piece_rows = positions // PIECES
    mix_steps = positions // STEP_ROWS
    scaling = HD ** (-0.5)
    contract = (((1,), (1,)), ((), ()))

    device = lax.axis_index("kv")
    z = device // columns
    x = lax.rem(device, columns)
    me = lax.axis_index("tp")
    core = lax.rem(me, 2)
    chip = me // 2
    chips = tp // 2
    partner = me + 1 - 2 * core

    def live_at(r):
        return sum([(r < reach[j]).astype(jnp.int32) for j in range(slots)])

    def column(i):
        return lax.rem(x + i, columns)

    def twin(off):
        return lax.rem(chip + off, chips) * 2 + core

    mine = live_at(device)
    row_live = live_at(z * columns)
    next_live = live_at((z + 1) * columns)

    loads = [
        pltpu.make_async_copy(wk_hbm, wkv_ref.at[:, pl.ds(0, half)], load_sem.at[0]),
        pltpu.make_async_copy(wv_hbm, wkv_ref.at[:, pl.ds(half, half)], load_sem.at[1]),
        pltpu.make_async_copy(wq_hbm, wq_ref, load_sem.at[2]),
        pltpu.make_async_copy(wo_hbm, wo_ref, load_sem.at[3]),
    ]

    def x_load(b):
        return pltpu.make_async_copy(x_hbm.at[b], x_ref.at[b], load_sem.at[4 + b])

    loads[0].start()
    loads[1].start()
    for b in range(batch_size):
        x_load(b).start()
    loads[2].start()
    loads[3].start()

    barrier = pltpu.get_barrier_semaphore()

    def greet(**where):
        pl.semaphore_signal(barrier, inc=1, device_id=where, device_id_type=MESH)

    greet(tp=partner)
    for off in range(1, chips):
        greet(tp=twin(off))
    for i in range(1, columns):
        greet(kv=z * columns + column(i))

    @pl.when(z > 0)
    def _():
        greet(kv=device - columns)

    @pl.when(z < rows_z - 1)
    def _():
        greet(kv=device + columns)

    lengths = [length_ref[b] for b in range(batch_size)]
    ranks = []
    for b in range(batch_size):
        ahead = [
            (lengths[o] >= lengths[b] if o < b else lengths[o] > lengths[b]).astype(jnp.int32)
            for o in range(batch_size) if o != b
        ]
        ranks.append(sum(ahead))

    def holder(j):
        return sum([jnp.where(ranks[b] == j, b, 0) for b in range(batch_size)])

    loads[0].wait()
    loads[1].wait()

    def project_kv(b, carry):
        x_load(b).wait()
        stage_ref[b] = jnp.dot(
            x_ref[b], wkv_ref[...], preferred_element_type=jnp.float32
        ).astype(jnp.bfloat16)
        return carry

    lax.fori_loop(0, batch_size, project_kv, 0)
    pl.semaphore_wait(
        barrier,
        chips + columns - 1
        + (z > 0).astype(jnp.int32) + (z < rows_z - 1).astype(jnp.int32),
    )

    def piece(j, c, p):
        return kv_ref.at[j, c, pl.ds(p * piece_rows, piece_rows)]

    def z_copy(j, c, p):
        return pltpu.make_async_remote_copy(
            src_ref=piece(j, c, p), dst_ref=piece(j, c, p),
            send_sem=z_sent.at[j, c // columns, p], recv_sem=got.at[j, c, p],
            device_id={"kv": device + columns}, device_id_type=MESH,
        )

    def x_copy(j, c, p, i):
        return pltpu.make_async_remote_copy(
            src_ref=piece(j, c, p), dst_ref=piece(j, c, p),
            send_sem=x_sent.at[j, c // columns, i - 1, p], recv_sem=got.at[j, c, p],
            device_id={"kv": z * columns + column(i)}, device_id_type=MESH,
        )

    def arrival(j, c, p):
        return pltpu.make_async_remote_copy(
            src_ref=piece(j, c, p), dst_ref=piece(j, c, p),
            send_sem=z_sent.at[j, c // columns, p], recv_sem=got.at[j, c, p],
            device_id={"tp": partner}, device_id_type=MESH,
        )

    def each_send(j, c, p, act):
        own = c == device

        @pl.when(j < next_live)
        def _():
            act(z_copy(j, c, p))

        for i in range(1, columns):
            wanted = (j < live_at(z * columns + column(i))) & (
                jnp.logical_not(own) | (column(i) > x)
            )

            @pl.when(wanted)
            def _():
                act(x_copy(j, c, p, i))

    def send_own(j):
        kv_ref[j, device] = stage_ref[holder(j)]
        for p in range(PIECES):
            each_send(j, device, p, lambda copy: copy.start())

    send_own(0)

    loads[2].wait()

    def project_q(b, carry):
        queries = jnp.dot(
            x_ref[b], wq_ref[...], preferred_element_type=jnp.float32
        ).astype(jnp.bfloat16)
        for n in range(kv_local * per_group):
            q_ref[b, n // per_group, pl.ds(lax.rem(n, per_group) * positions, positions), :] = (
                queries[:, n * HD:(n + 1) * HD]
            )
        return carry

    lax.fori_loop(0, batch_size, project_q, 0)
    loads[3].wait()

    def named(names, c):
        segment = lax.broadcasted_iota(jnp.int32, (per_dev, positions), 1) // KB
        bias = jnp.full((per_dev, positions), MASKED, jnp.float32)
        for i in range(per_dev):
            hit = jnp.max(
                jnp.where(names == c * per_dev + i, 0.0, MASKED), axis=1, keepdims=True
            )
            bias = jnp.where(segment == i, hit, bias)
        return jnp.broadcast_to(bias[:, None, :], (per_dev, KB, positions)).reshape(
            positions, positions
        )

    def scores(b, j, c, h, bias):
        raw = lax.dot_general(
            q_ref[b, h], kv_ref[j, c, :, h * HD:(h + 1) * HD], contract,
            preferred_element_type=jnp.float32,
        )
        shaped = (raw * scaling).reshape(per_group, positions, positions) + bias[None]
        return shaped.reshape(rows, positions)

    def weigh(j, c, h, raised):
        return jnp.dot(
            raised.astype(jnp.bfloat16), kv_ref[j, c, :, half + h * HD:half + (h + 1) * HD],
            preferred_element_type=jnp.float32,
        )

    def wide(value):
        return jnp.concatenate([value] * (positions // HD), axis=1)

    def attend_own(j):
        b = holder(j)
        names = chosen_ref[b]
        before = named(names, device)
        home = device * per_dev + lax.broadcasted_iota(jnp.int32, names.shape, 0)
        copies = jnp.sum(jnp.where(names == home, 1.0, 0.0), axis=1, keepdims=True)
        same = jnp.log(jnp.maximum(copies, 1.0))
        same = jnp.broadcast_to(same[:, None, :], (per_dev, KB, positions)).reshape(
            positions, positions
        )
        at_row = lax.broadcasted_iota(jnp.int32, (positions, positions), 0)
        at_col = lax.broadcasted_iota(jnp.int32, (positions, positions), 1)
        bias = jnp.where(at_col < at_row, before, jnp.where(at_col == at_row, same, MASKED))
        for h in range(kv_local):
            s = scores(b, j, device, h, bias)
            top = jnp.broadcast_to(jnp.max(s, axis=1, keepdims=True), (rows, HD))
            raised = jnp.exp(s - wide(top))
            top_ref[h] = top
            total_ref[h] = jnp.broadcast_to(jnp.sum(raised, axis=1, keepdims=True), (rows, HD))
            acc_ref[h] = weigh(j, device, h, raised)

    def attend_far(j, c):
        b = holder(j)
        bias = named(chosen_ref[b], c)
        for h in range(kv_local):
            s = scores(b, j, c, h, bias)
            old = top_ref[h]
            top = jnp.maximum(old, jnp.max(s, axis=1, keepdims=True))
            fade = jnp.exp(old - top)
            raised = jnp.exp(s - wide(top))
            top_ref[h] = top
            total_ref[h] = total_ref[h] * fade + jnp.sum(raised, axis=1, keepdims=True)
            acc_ref[h] = acc_ref[h] * fade + weigh(j, c, h, raised)

    def attend_end(j):
        live = sum(
            [jnp.where(ranks[b] == j, lengths[b], 0) for b in range(batch_size)]
        ) - device * positions
        living = lax.broadcasted_iota(jnp.int32, (positions, HD), 0) < live
        for h in range(kv_local):
            done = acc_ref[h] / total_ref[h]
            for g in range(per_group):
                n = h * per_group + g
                att_ref[j, :, n * HD:(n + 1) * HD] = jnp.where(
                    living, done[g * positions:(g + 1) * positions], 0.0
                ).astype(jnp.bfloat16)

    def group_sum(j, m, off, side):
        start = (lax.rem(chip + off, chips) * 2 + side) * width
        return jnp.dot(
            att_ref[j, m * STEP_ROWS:(m + 1) * STEP_ROWS, :],
            wo_ref[:, pl.ds(pl.multiple_of(start, width), width)],
            preferred_element_type=jnp.float32,
        ).astype(jnp.bfloat16)

    def pair_copy(i):
        return pltpu.make_async_remote_copy(
            src_ref=pair_out.at[i], dst_ref=pair_in.at[i],
            send_sem=pair_sent.at[i], recv_sem=pair_got.at[i],
            device_id={"tp": partner}, device_id_type=MESH,
        )

    def far_copy(i, off):
        return pltpu.make_async_remote_copy(
            src_ref=far_out.at[off - 1, i], dst_ref=far_in.at[off - 1, i],
            send_sem=far_sent.at[off - 1, i], recv_sem=far_got.at[off - 1, i],
            device_id={"tp": twin(off)}, device_id_type=MESH,
        )

    def mix(j):
        for m in range(mix_steps):
            i = j * mix_steps + m
            for off in range(chips):
                pair_out[i, off] = group_sum(j, m, off, 1 - core)
            pair_copy(i).start()
        for m in range(mix_steps):
            i = j * mix_steps + m
            sums = [group_sum(j, m, off, core).astype(jnp.float32) for off in range(chips)]
            pair_copy(i).wait_recv()
            for off in range(1, chips):
                both = sums[off] + pair_in[i, off].astype(jnp.float32)
                far_out[off - 1, i] = both.astype(jnp.bfloat16)
                far_copy(i, off).start()
            near[i] = sums[0] + pair_in[i, 0].astype(jnp.float32)

    def slot(j, carry):
        used = j < mine

        @pl.when(used)
        def _():
            attend_own(j)

        def step(t, carry):
            d = t // columns
            i = lax.rem(t, columns)
            c = (z - d) * columns + column(i)
            relayed = (i == 0) & (d > 0)
            taken = used & (i > 0) & ((d > 0) | (column(i) < x))

            @pl.when(relayed)
            def _():
                for p in range(PIECES):
                    arrival(j, c, p).wait_recv()
                    each_send(j, c, p, lambda copy: copy.start())

            @pl.when(taken)
            def _():
                for p in range(PIECES):
                    arrival(j, c, p).wait_recv()

            @pl.when((relayed & used) | taken)
            def _():
                attend_far(j, c)

            return carry

        lax.fori_loop(0, (z + 1) * columns, step, 0)

        @pl.when(j + 1 < row_live)
        def _():
            send_own(j + 1)

        @pl.when(used)
        def _():
            attend_end(j)
            mix(j)

        return carry

    lax.fori_loop(0, row_live, slot, 0)

    def finish(j, carry):
        for m in range(mix_steps):
            i = j * mix_steps + m
            pair_copy(i).wait_send()
            mixed = near[i]
            for off in range(1, chips):
                far_copy(i, off).wait()
                mixed = mixed + far_in[off - 1, i].astype(jnp.float32)
            mixed_ref[j, m * STEP_ROWS:(m + 1) * STEP_ROWS, :] = mixed.astype(jnp.bfloat16)
        return carry

    lax.fori_loop(0, mine, finish, 0)

    def blank(j, carry):
        mixed_ref[j] = jnp.zeros(mixed_ref.shape[1:], jnp.bfloat16)
        return carry

    lax.fori_loop(mine, slots, blank, 0)
    for b in range(batch_size):
        out_ref[b] = mixed_ref[ranks[b]]

    def drain(j, carry):
        def back(d, carry):
            c = (z - d) * columns + x
            for p in range(PIECES):
                each_send(j, c, p, lambda copy: copy.wait_send())
            return carry

        return lax.fori_loop(0, z + 1, back, carry)

    lax.fori_loop(0, row_live, drain, 0)


def columns_of(devices):
    return 1 << ((devices.bit_length() - 1) // 2)


def shards(inputs, query_weight, key_weight, value_weight, out_weight, chosen, lengths):
    batch_size, positions, model_width = inputs.shape
    kv_local = key_weight.shape[1] // HD
    heads_local = query_weight.shape[1] // HD
    per_group = heads_local // kv_local
    devices = lax.axis_size("kv")
    tp = lax.axis_size("tp")
    chips = tp // 2
    columns = columns_of(devices)
    reach = spans(batch_size, devices, positions)
    width = out_weight.shape[1] // tp
    steps = batch_size * (positions // STEP_ROWS)
    rows = per_group * positions
    bf16, f32 = jnp.bfloat16, jnp.float32
    vmem = pl.BlockSpec(memory_space=pltpu.VMEM)
    hbm = pl.BlockSpec(memory_space=pl.ANY)
    dma = pltpu.SemaphoreType.DMA
    pair = pltpu.VMEM((steps, chips, STEP_ROWS, width), bf16)
    far = pltpu.VMEM((chips - 1, steps, STEP_ROWS, width), bf16)
    return pl.pallas_call(
        functools.partial(layer_kernel, reach, columns, kv_local, per_group, tp),
        out_shape=jax.ShapeDtypeStruct((batch_size, positions, width), bf16),
        in_specs=[pl.BlockSpec(memory_space=pltpu.SMEM)] + [hbm] * 5 + [vmem],
        out_specs=vmem,
        scratch_shapes=[
            pltpu.VMEM(inputs.shape, bf16),
            pltpu.VMEM(query_weight.shape, bf16),
            pltpu.VMEM((model_width, 2 * kv_local * HD), bf16),
            pltpu.VMEM(out_weight.shape, bf16),
            pltpu.VMEM((batch_size, positions, 2 * kv_local * HD), bf16),
            pltpu.VMEM((batch_size, devices, positions, 2 * kv_local * HD), bf16),
            pltpu.VMEM((batch_size, kv_local, rows, HD), bf16),
            pltpu.VMEM((kv_local, rows, HD), f32),
            pltpu.VMEM((kv_local, rows, HD), f32),
            pltpu.VMEM((kv_local, rows, HD), f32),
            pltpu.VMEM((batch_size, positions, heads_local * HD), bf16),
            pair, pair, far, far,
            pltpu.VMEM((steps, STEP_ROWS, width), f32),
            pltpu.VMEM((batch_size, positions, width), bf16),
            dma((4 + batch_size,)),
            dma((batch_size, devices // columns, PIECES)),
            dma((batch_size, devices // columns, max(columns - 1, 1), PIECES)),
            dma((batch_size, devices, PIECES)),
            dma((steps,)), dma((steps,)),
            dma((chips - 1, steps)), dma((chips - 1, steps)),
        ],
        compiler_params=pltpu.CompilerParams(
            collective_id=0, has_side_effects=True, vmem_limit_bytes=60 * 2**20
        ),
    )(lengths, inputs, query_weight, key_weight, value_weight, out_weight, chosen)


def solution(mesh):
    placed = (
        P(None, "kv", None),
        P(None, "tp"),
        P(None, "tp"),
        P(None, "tp"),
        P("tp", None),
        P(None, "kv", None),
        P(),
    )
    return jax.shard_map(
        shards, mesh=mesh, in_specs=placed, out_specs=P(None, "kv", "tp"), check_vma=False
    )
```

```python
import functools

import jax
import jax.numpy as jnp
from jax import lax
from jax.experimental import pallas as pl
from jax.experimental.pallas import tpu as pltpu
from jax.sharding import PartitionSpec as P

HD = 128
KB = 64
MASKED = -1e30
PIECES = 2
STEP_ROWS = 128
MESH = pl.DeviceIdType.MESH


def spans(batch_size, devices, positions):
    seq = devices * positions
    total = seq + seq // 2
    longest = [min(seq, (total - (batch_size - 1 - j)) // (j + 1)) for j in range(batch_size)]
    whole = tuple(-(-length // positions) for length in longest)
    short = tuple(
        min(full, -(-devices * 3 // (8 * j)) if j else devices) for j, full in enumerate(whole)
    )
    return short, whole


def layer_kernel(
    reach, columns, kv_local, per_group, tp,
    length_ref, x_hbm, wq_hbm, wk_hbm, wv_hbm, wo_hbm, chosen_ref, out_ref,
    x_ref, wq_ref, wkv_ref, wo_ref, kv_ref, q_ref,
    top_ref, total_ref, acc_ref, att_ref,
    pair_out, pair_in, far_out, far_in, near, mixed_ref,
    load_sem, z_sent, x_sent, got, pair_sent, pair_got, far_sent, far_got,
):
    batch_size, positions, _ = x_ref.shape
    slots, devices = kv_ref.shape[:2]
    rows_z = devices // columns
    per_dev = positions // KB
    half = kv_local * HD
    rows = per_group * positions
    width = out_ref.shape[-1]
    piece_rows = positions // PIECES
    mix_steps = positions // STEP_ROWS
    scaling = HD ** (-0.5)
    contract = (((1,), (1,)), ((), ()))

    device = lax.axis_index("kv")
    z = device // columns
    x = lax.rem(device, columns)
    me = lax.axis_index("tp")
    core = lax.rem(me, 2)
    chip = me // 2
    chips = tp // 2
    partner = me + 1 - 2 * core

    def live_at(r):
        return sum([(r < reach[j]).astype(jnp.int32) for j in range(slots)])

    def column(i):
        return lax.rem(x + i, columns)

    def twin(off):
        return lax.rem(chip + off, chips) * 2 + core

    mine = live_at(device)
    row_live = live_at(z * columns)
    next_live = live_at((z + 1) * columns)

    loads = [
        pltpu.make_async_copy(wk_hbm, wkv_ref.at[:, pl.ds(0, half)], load_sem.at[0]),
        pltpu.make_async_copy(wv_hbm, wkv_ref.at[:, pl.ds(half, half)], load_sem.at[1]),
        pltpu.make_async_copy(wq_hbm, wq_ref, load_sem.at[2]),
        pltpu.make_async_copy(wo_hbm, wo_ref, load_sem.at[3]),
    ]

    def x_load(b):
        return pltpu.make_async_copy(x_hbm.at[b], x_ref.at[b], load_sem.at[4 + b])

    loads[0].start()
    loads[1].start()
    for b in range(batch_size):
        x_load(b).start()
    loads[2].start()
    loads[3].start()

    barrier = pltpu.get_barrier_semaphore()

    def greet(**where):
        pl.semaphore_signal(barrier, inc=1, device_id=where, device_id_type=MESH)

    greet(tp=partner)
    for off in range(1, chips):
        greet(tp=twin(off))
    for i in range(1, columns):
        greet(kv=z * columns + column(i))

    @pl.when(z > 0)
    def _():
        greet(kv=device - columns)

    @pl.when(z < rows_z - 1)
    def _():
        greet(kv=device + columns)

    lengths = [length_ref[b] for b in range(batch_size)]
    ranks = []
    for b in range(batch_size):
        ahead = [
            (lengths[o] >= lengths[b] if o < b else lengths[o] > lengths[b]).astype(jnp.int32)
            for o in range(batch_size) if o != b
        ]
        ranks.append(sum(ahead))

    def holder(j):
        return sum([jnp.where(ranks[b] == j, b, 0) for b in range(batch_size)])

    pl.semaphore_wait(
        barrier,
        chips + columns - 1
        + (z > 0).astype(jnp.int32) + (z < rows_z - 1).astype(jnp.int32),
    )

    def piece(j, c, p):
        return kv_ref.at[j, c, pl.ds(p * piece_rows, piece_rows)]

    def z_copy(j, c, p):
        return pltpu.make_async_remote_copy(
            src_ref=piece(j, c, p), dst_ref=piece(j, c, p),
            send_sem=z_sent.at[j, c // columns, p], recv_sem=got.at[j, c, p],
            device_id={"kv": device + columns}, device_id_type=MESH,
        )

    def x_copy(j, c, p, i):
        return pltpu.make_async_remote_copy(
            src_ref=piece(j, c, p), dst_ref=piece(j, c, p),
            send_sem=x_sent.at[j, c // columns, i - 1, p], recv_sem=got.at[j, c, p],
            device_id={"kv": z * columns + column(i)}, device_id_type=MESH,
        )

    def arrival(j, c, p):
        return pltpu.make_async_remote_copy(
            src_ref=piece(j, c, p), dst_ref=piece(j, c, p),
            send_sem=z_sent.at[j, c // columns, p], recv_sem=got.at[j, c, p],
            device_id={"tp": partner}, device_id_type=MESH,
        )

    def each_send(j, c, p, act):
        own = c == device

        @pl.when(j < next_live)
        def _():
            act(z_copy(j, c, p))

        for i in range(1, columns):
            wanted = (j < live_at(z * columns + column(i))) & (
                jnp.logical_not(own) | (column(i) > x)
            )

            @pl.when(wanted)
            def _():
                act(x_copy(j, c, p, i))

    def send_own(j):
        for p in range(PIECES):
            each_send(j, device, p, lambda copy: copy.start())

    loads[0].wait()
    loads[1].wait()
    for b in range(batch_size):
        x_load(b).wait()

    def project_kv(j, carry):
        kv_ref[j, device] = jnp.dot(
            x_ref[holder(j)], wkv_ref[...], preferred_element_type=jnp.float32
        ).astype(jnp.bfloat16)

        @pl.when((j == 0) | (z == 0))
        def _():
            send_own(j)

        return carry

    lax.fori_loop(0, row_live, project_kv, 0)
    loads[2].wait()
    loads[3].wait()

    def project_q(j):
        queries = jnp.dot(
            x_ref[holder(j)], wq_ref[...], preferred_element_type=jnp.float32
        ).astype(jnp.bfloat16)
        for n in range(kv_local * per_group):
            h, g = n // per_group, n % per_group
            q_ref[h, g * positions:(g + 1) * positions, :] = queries[:, n * HD:(n + 1) * HD]

    def named(names, c):
        segment = lax.broadcasted_iota(jnp.int32, (per_dev, positions), 1) // KB
        bias = jnp.full((per_dev, positions), MASKED, jnp.float32)
        for i in range(per_dev):
            hit = jnp.max(
                jnp.where(names == c * per_dev + i, 0.0, MASKED), axis=1, keepdims=True
            )
            bias = jnp.where(segment == i, hit, bias)
        return jnp.broadcast_to(bias[:, None, :], (per_dev, KB, positions)).reshape(
            positions, positions
        )

    def scores(j, c, h, bias):
        raw = lax.dot_general(
            q_ref[h], kv_ref[j, c, :, h * HD:(h + 1) * HD], contract,
            preferred_element_type=jnp.float32,
        )
        shaped = (raw * scaling).reshape(per_group, positions, positions) + bias[None]
        return shaped.reshape(rows, positions)

    def weigh(j, c, h, raised):
        return jnp.dot(
            raised.astype(jnp.bfloat16), kv_ref[j, c, :, half + h * HD:half + (h + 1) * HD],
            preferred_element_type=jnp.float32,
        )

    def wide(value):
        return jnp.concatenate([value] * (positions // HD), axis=1)

    def attend_own(j):
        names = chosen_ref[holder(j)]
        before = named(names, device)
        home = device * per_dev + lax.broadcasted_iota(jnp.int32, names.shape, 0)
        copies = jnp.sum(jnp.where(names == home, 1.0, 0.0), axis=1, keepdims=True)
        same = jnp.log(jnp.maximum(copies, 1.0))
        same = jnp.broadcast_to(same[:, None, :], (per_dev, KB, positions)).reshape(
            positions, positions
        )
        at_row = lax.broadcasted_iota(jnp.int32, (positions, positions), 0)
        at_col = lax.broadcasted_iota(jnp.int32, (positions, positions), 1)
        bias = jnp.where(at_col < at_row, before, jnp.where(at_col == at_row, same, MASKED))
        for h in range(kv_local):
            s = scores(j, device, h, bias)
            top = jnp.broadcast_to(jnp.max(s, axis=1, keepdims=True), (rows, HD))
            raised = jnp.exp(s - wide(top))
            top_ref[h] = top
            total_ref[h] = jnp.broadcast_to(jnp.sum(raised, axis=1, keepdims=True), (rows, HD))
            acc_ref[h] = weigh(j, device, h, raised)

    def attend_far(j, c):
        bias = named(chosen_ref[holder(j)], c)
        for h in range(kv_local):
            s = scores(j, c, h, bias)
            old = top_ref[h]
            top = jnp.maximum(old, jnp.max(s, axis=1, keepdims=True))
            fade = jnp.exp(old - top)
            raised = jnp.exp(s - wide(top))
            top_ref[h] = top
            total_ref[h] = total_ref[h] * fade + jnp.sum(raised, axis=1, keepdims=True)
            acc_ref[h] = acc_ref[h] * fade + weigh(j, c, h, raised)

    def attend_end(j):
        live = sum(
            [jnp.where(ranks[b] == j, lengths[b], 0) for b in range(batch_size)]
        ) - device * positions
        living = lax.broadcasted_iota(jnp.int32, (positions, HD), 0) < live
        for h in range(kv_local):
            done = acc_ref[h] / total_ref[h]
            for g in range(per_group):
                n = h * per_group + g
                att_ref[j, :, n * HD:(n + 1) * HD] = jnp.where(
                    living, done[g * positions:(g + 1) * positions], 0.0
                ).astype(jnp.bfloat16)

    def group_sum(j, m, off, side):
        start = (lax.rem(chip + off, chips) * 2 + side) * width
        return jnp.dot(
            att_ref[j, m * STEP_ROWS:(m + 1) * STEP_ROWS, :],
            wo_ref[:, pl.ds(pl.multiple_of(start, width), width)],
            preferred_element_type=jnp.float32,
        ).astype(jnp.bfloat16)

    def pair_copy(i):
        return pltpu.make_async_remote_copy(
            src_ref=pair_out.at[i], dst_ref=pair_in.at[i],
            send_sem=pair_sent.at[i], recv_sem=pair_got.at[i],
            device_id={"tp": partner}, device_id_type=MESH,
        )

    def far_copy(i, off):
        return pltpu.make_async_remote_copy(
            src_ref=far_out.at[off - 1, i], dst_ref=far_in.at[off - 1, i],
            send_sem=far_sent.at[off - 1, i], recv_sem=far_got.at[off - 1, i],
            device_id={"tp": twin(off)}, device_id_type=MESH,
        )

    def mix(j):
        for m in range(mix_steps):
            i = j * mix_steps + m
            for off in range(chips):
                pair_out[i, off] = group_sum(j, m, off, 1 - core)
            pair_copy(i).start()
        for m in range(mix_steps):
            i = j * mix_steps + m
            sums = [group_sum(j, m, off, core).astype(jnp.float32) for off in range(chips)]
            pair_copy(i).wait_recv()
            for off in range(1, chips):
                both = sums[off] + pair_in[i, off].astype(jnp.float32)
                far_out[off - 1, i] = both.astype(jnp.bfloat16)
                far_copy(i, off).start()
            near[i] = sums[0] + pair_in[i, 0].astype(jnp.float32)

    def relay(t):
        j = t // z
        d = lax.rem(t, z)
        c = device - (d + 1) * columns

        @pl.when((d == 0) & (j > 0))
        def _():
            send_own(j)

        for p in range(PIECES):
            arrival(j, c, p).wait_recv()
            each_send(j, c, p, lambda copy: copy.start())

    def take(j, c):
        for p in range(PIECES):
            arrival(j, c, p).wait_recv()
        attend_far(j, c)

    def slot(j, carry):
        used = j < mine

        @pl.when(used)
        def _():
            project_q(j)
            attend_own(j)

        @pl.when((j == 0) & (z > 0))
        def _():
            relay(0)

        def step(t, carry):
            d = t // columns
            i = lax.rem(t, columns)
            c = (z - d) * columns + column(i)
            ahead = j * z + d

            @pl.when((i == 0) & (d > 0) & (ahead < row_live * z))
            def _():
                relay(ahead)

            @pl.when(used & (i == 0) & (d > 0))
            def _():
                attend_far(j, c)

            @pl.when(used & (i > 0) & ((d > 0) | (column(i) < x)))
            def _():
                take(j, c)

            return carry

        lax.fori_loop(0, (z + 1) * columns, step, 0)

        @pl.when(used)
        def _():
            attend_end(j)
            mix(j)

        return carry

    lax.fori_loop(0, row_live, slot, 0)

    def finish(j, carry):
        for m in range(mix_steps):
            i = j * mix_steps + m
            pair_copy(i).wait_send()
            mixed = near[i]
            for off in range(1, chips):
                far_copy(i, off).wait()
                mixed = mixed + far_in[off - 1, i].astype(jnp.float32)
            mixed_ref[j, m * STEP_ROWS:(m + 1) * STEP_ROWS, :] = mixed.astype(jnp.bfloat16)
        return carry

    lax.fori_loop(0, mine, finish, 0)

    def blank(j, carry):
        mixed_ref[j] = jnp.zeros(mixed_ref.shape[1:], jnp.bfloat16)
        return carry

    lax.fori_loop(mine, slots, blank, 0)
    for b in range(batch_size):
        out_ref[b] = mixed_ref[ranks[b]]

    def drain(j, carry):
        def back(d, carry):
            c = (z - d) * columns + x
            for p in range(PIECES):
                each_send(j, c, p, lambda copy: copy.wait_send())
            return carry

        return lax.fori_loop(0, z + 1, back, carry)

    lax.fori_loop(0, row_live, drain, 0)


def columns_of(devices):
    return 1 << ((devices.bit_length() - 1) // 2)


def layer(
    reach, collective_id,
    inputs, query_weight, key_weight, value_weight, out_weight, chosen, lengths,
):
    batch_size, positions, model_width = inputs.shape
    kv_local = key_weight.shape[1] // HD
    heads_local = query_weight.shape[1] // HD
    per_group = heads_local // kv_local
    devices = lax.axis_size("kv")
    tp = lax.axis_size("tp")
    chips = tp // 2
    columns = columns_of(devices)
    width = out_weight.shape[1] // tp
    steps = batch_size * (positions // STEP_ROWS)
    rows = per_group * positions
    bf16, f32 = jnp.bfloat16, jnp.float32
    vmem = pl.BlockSpec(memory_space=pltpu.VMEM)
    hbm = pl.BlockSpec(memory_space=pl.ANY)
    dma = pltpu.SemaphoreType.DMA
    pair = pltpu.VMEM((steps, chips, STEP_ROWS, width), bf16)
    far = pltpu.VMEM((chips - 1, steps, STEP_ROWS, width), bf16)
    return pl.pallas_call(
        functools.partial(layer_kernel, reach, columns, kv_local, per_group, tp),
        out_shape=jax.ShapeDtypeStruct((batch_size, positions, width), bf16),
        in_specs=[pl.BlockSpec(memory_space=pltpu.SMEM)] + [hbm] * 5 + [vmem],
        out_specs=vmem,
        scratch_shapes=[
            pltpu.VMEM(inputs.shape, bf16),
            pltpu.VMEM(query_weight.shape, bf16),
            pltpu.VMEM((model_width, 2 * kv_local * HD), bf16),
            pltpu.VMEM(out_weight.shape, bf16),
            pltpu.VMEM((batch_size, devices, positions, 2 * kv_local * HD), bf16),
            pltpu.VMEM((kv_local, rows, HD), bf16),
            pltpu.VMEM((kv_local, rows, HD), f32),
            pltpu.VMEM((kv_local, rows, HD), f32),
            pltpu.VMEM((kv_local, rows, HD), f32),
            pltpu.VMEM((batch_size, positions, heads_local * HD), bf16),
            pair, pair, far, far,
            pltpu.VMEM((steps, STEP_ROWS, width), f32),
            pltpu.VMEM((batch_size, positions, width), bf16),
            dma((4 + batch_size,)),
            dma((batch_size, devices // columns, PIECES)),
            dma((batch_size, devices // columns, max(columns - 1, 1), PIECES)),
            dma((batch_size, devices, PIECES)),
            dma((steps,)), dma((steps,)),
            dma((chips - 1, steps)), dma((chips - 1, steps)),
        ],
        compiler_params=pltpu.CompilerParams(
            collective_id=collective_id, has_side_effects=True, vmem_limit_bytes=60 * 2**20
        ),
    )(lengths, inputs, query_weight, key_weight, value_weight, out_weight, chosen)


def shards(*args):
    inputs, lengths = args[0], args[-1]
    batch_size, positions, _ = inputs.shape
    short, whole = spans(batch_size, lax.axis_size("kv"), positions)
    longer = [jnp.sum(lengths > span * positions) <= j for j, span in enumerate(short)]
    return lax.cond(
        functools.reduce(jnp.logical_and, longer),
        functools.partial(layer, short, 0),
        functools.partial(layer, whole, 1),
        *args,
    )


def solution(mesh):
    placed = (
        P(None, "kv", None),
        P(None, "tp"),
        P(None, "tp"),
        P(None, "tp"),
        P("tp", None),
        P(None, "kv", None),
        P(),
    )
    return jax.shard_map(
        shards, mesh=mesh, in_specs=placed, out_specs=P(None, "kv", "tp"), check_vma=False
    )
```

```python
import functools

import jax
import jax.numpy as jnp
from jax import lax
from jax.experimental import pallas as pl
from jax.experimental.pallas import tpu as pltpu
from jax.sharding import PartitionSpec as P

HD = 128
KB = 64
MASKED = -1e30
PIECES = 2
STEP_ROWS = 128
MESH = pl.DeviceIdType.MESH


def spans(batch_size, devices, positions):
    seq = devices * positions
    total = seq + seq // 2
    longest = [min(seq, (total - (batch_size - 1 - j)) // (j + 1)) for j in range(batch_size)]
    whole = tuple(-(-length // positions) for length in longest)
    short = tuple(
        min(full, -(-devices * 3 // (8 * j)) if j else devices) for j, full in enumerate(whole)
    )
    return short, whole


def layer_kernel(
    reach, columns, kv_local, per_group, tp,
    length_hbm, x_hbm, wq_hbm, wk_hbm, wv_hbm, wo_hbm, chosen_hbm, out_ref,
    length_ref, chosen_ref, x_ref, wq_ref, wkv_ref, wo_ref, kv_ref, q_ref,
    top_ref, total_ref, acc_ref, att_ref,
    pair_out, pair_in, far_out, far_in, near, mixed_ref,
    load_sem, z_sent, x_sent, got, pair_sent, pair_got, far_sent, far_got,
):
    batch_size, positions, _ = x_ref.shape
    slots, devices = kv_ref.shape[:2]
    rows_z = devices // columns
    per_dev = positions // KB
    half = kv_local * HD
    rows = per_group * positions
    width = out_ref.shape[-1]
    piece_rows = positions // PIECES
    mix_steps = positions // STEP_ROWS
    scaling = HD ** (-0.5)
    contract = (((1,), (1,)), ((), ()))

    device = lax.axis_index("kv")
    z = device // columns
    x = lax.rem(device, columns)
    me = lax.axis_index("tp")
    core = lax.rem(me, 2)
    chip = me // 2
    chips = tp // 2
    partner = me + 1 - 2 * core

    def live_at(r):
        return sum([(r < reach[j]).astype(jnp.int32) for j in range(slots)])

    def column(i):
        return lax.rem(x + i, columns)

    def twin(off):
        return lax.rem(chip + off, chips) * 2 + core

    mine = live_at(device)
    row_live = live_at(z * columns)
    next_live = live_at((z + 1) * columns)

    loads = [
        pltpu.make_async_copy(wk_hbm, wkv_ref.at[:, pl.ds(0, half)], load_sem.at[0]),
        pltpu.make_async_copy(wv_hbm, wkv_ref.at[:, pl.ds(half, half)], load_sem.at[1]),
        pltpu.make_async_copy(wq_hbm, wq_ref, load_sem.at[2]),
        pltpu.make_async_copy(wo_hbm, wo_ref, load_sem.at[3]),
        pltpu.make_async_copy(length_hbm, length_ref, load_sem.at[4]),
        pltpu.make_async_copy(chosen_hbm, chosen_ref, load_sem.at[5]),
    ]

    def x_load(b):
        return pltpu.make_async_copy(x_hbm.at[b], x_ref.at[b], load_sem.at[6 + b])

    loads[4].start()
    for b in range(batch_size):
        x_load(b).start()
    loads[0].start()
    loads[1].start()
    loads[5].start()

    barrier = pltpu.get_barrier_semaphore()

    def greet(**where):
        pl.semaphore_signal(barrier, inc=1, device_id=where, device_id_type=MESH)

    greet(tp=partner)
    for off in range(1, chips):
        greet(tp=twin(off))
    for i in range(1, columns):
        greet(kv=z * columns + column(i))

    @pl.when(z > 0)
    def _():
        greet(kv=device - columns)

    @pl.when(z < rows_z - 1)
    def _():
        greet(kv=device + columns)

    loads[4].wait()
    lengths = [length_ref[b] for b in range(batch_size)]
    ranks = []
    for b in range(batch_size):
        ahead = [
            (lengths[o] >= lengths[b] if o < b else lengths[o] > lengths[b]).astype(jnp.int32)
            for o in range(batch_size) if o != b
        ]
        ranks.append(sum(ahead))

    def holder(j):
        return sum([jnp.where(ranks[b] == j, b, 0) for b in range(batch_size)])

    def piece(j, c, p):
        return kv_ref.at[j, c, pl.ds(p * piece_rows, piece_rows)]

    def z_copy(j, c, p):
        return pltpu.make_async_remote_copy(
            src_ref=piece(j, c, p), dst_ref=piece(j, c, p),
            send_sem=z_sent.at[j, c // columns, p], recv_sem=got.at[j, c, p],
            device_id={"kv": device + columns}, device_id_type=MESH,
        )

    def x_copy(j, c, p, i):
        return pltpu.make_async_remote_copy(
            src_ref=piece(j, c, p), dst_ref=piece(j, c, p),
            send_sem=x_sent.at[j, c // columns, i - 1, p], recv_sem=got.at[j, c, p],
            device_id={"kv": z * columns + column(i)}, device_id_type=MESH,
        )

    def arrival(j, c, p):
        return pltpu.make_async_remote_copy(
            src_ref=piece(j, c, p), dst_ref=piece(j, c, p),
            send_sem=z_sent.at[j, c // columns, p], recv_sem=got.at[j, c, p],
            device_id={"tp": partner}, device_id_type=MESH,
        )

    def each_send(j, c, p, act):
        own = c == device

        @pl.when(j < next_live)
        def _():
            act(z_copy(j, c, p))

        for i in range(1, columns):
            wanted = (j < live_at(z * columns + column(i))) & (
                jnp.logical_not(own) | (column(i) > x)
            )

            @pl.when(wanted)
            def _():
                act(x_copy(j, c, p, i))

    def send_own(j):
        for p in range(PIECES):
            each_send(j, device, p, lambda copy: copy.start())

    loads[0].wait()
    loads[1].wait()
    for b in range(batch_size):
        x_load(b).wait()

    loads[2].start()

    def project_kv(j, carry):
        kv_ref[j, device] = jnp.dot(
            x_ref[holder(j)], wkv_ref[...], preferred_element_type=jnp.float32
        ).astype(jnp.bfloat16)

        @pl.when(j == 0)
        def _():
            pl.semaphore_wait(
                barrier,
                chips + columns - 1
                + (z > 0).astype(jnp.int32) + (z < rows_z - 1).astype(jnp.int32),
            )

        @pl.when((j == 0) | (z == 0))
        def _():
            send_own(j)

        return carry

    lax.fori_loop(0, jnp.where(z == 0, 1, row_live), project_kv, 0)
    loads[3].start()
    loads[2].wait()
    loads[5].wait()

    def project_q(j):
        queries = jnp.dot(
            x_ref[holder(j)], wq_ref[...], preferred_element_type=jnp.float32
        ).astype(jnp.bfloat16)
        for n in range(kv_local * per_group):
            h, g = n // per_group, n % per_group
            q_ref[h, g * positions:(g + 1) * positions, :] = queries[:, n * HD:(n + 1) * HD]

    def named(names, c):
        segment = lax.broadcasted_iota(jnp.int32, (per_dev, positions), 1) // KB
        bias = jnp.full((per_dev, positions), MASKED, jnp.float32)
        for i in range(per_dev):
            hit = jnp.max(
                jnp.where(names == c * per_dev + i, 0.0, MASKED), axis=1, keepdims=True
            )
            bias = jnp.where(segment == i, hit, bias)
        return jnp.broadcast_to(bias[:, None, :], (per_dev, KB, positions)).reshape(
            positions, positions
        )

    def scores(j, c, h, bias):
        raw = lax.dot_general(
            q_ref[h], kv_ref[j, c, :, h * HD:(h + 1) * HD], contract,
            preferred_element_type=jnp.float32,
        )
        shaped = (raw * scaling).reshape(per_group, positions, positions) + bias[None]
        return shaped.reshape(rows, positions)

    def weigh(j, c, h, raised):
        return jnp.dot(
            raised.astype(jnp.bfloat16), kv_ref[j, c, :, half + h * HD:half + (h + 1) * HD],
            preferred_element_type=jnp.float32,
        )

    def wide(value):
        return jnp.concatenate([value] * (positions // HD), axis=1)

    def attend_own(j):
        names = chosen_ref[holder(j)]
        before = named(names, device)
        home = device * per_dev + lax.broadcasted_iota(jnp.int32, names.shape, 0)
        copies = jnp.sum(jnp.where(names == home, 1.0, 0.0), axis=1, keepdims=True)
        same = jnp.log(jnp.maximum(copies, 1.0))
        same = jnp.broadcast_to(same[:, None, :], (per_dev, KB, positions)).reshape(
            positions, positions
        )
        at_row = lax.broadcasted_iota(jnp.int32, (positions, positions), 0)
        at_col = lax.broadcasted_iota(jnp.int32, (positions, positions), 1)
        bias = jnp.where(at_col < at_row, before, jnp.where(at_col == at_row, same, MASKED))
        for h in range(kv_local):
            s = scores(j, device, h, bias)
            top = jnp.broadcast_to(jnp.max(s, axis=1, keepdims=True), (rows, HD))
            raised = jnp.exp(s - wide(top))
            top_ref[h] = top
            total_ref[h] = jnp.broadcast_to(jnp.sum(raised, axis=1, keepdims=True), (rows, HD))
            acc_ref[h] = weigh(j, device, h, raised)

    def attend_far(j, c):
        bias = named(chosen_ref[holder(j)], c)
        for h in range(kv_local):
            s = scores(j, c, h, bias)
            old = top_ref[h]
            top = jnp.maximum(old, jnp.max(s, axis=1, keepdims=True))
            fade = jnp.exp(old - top)
            raised = jnp.exp(s - wide(top))
            top_ref[h] = top
            total_ref[h] = total_ref[h] * fade + jnp.sum(raised, axis=1, keepdims=True)
            acc_ref[h] = acc_ref[h] * fade + weigh(j, c, h, raised)

    def attend_end(j):
        live = sum(
            [jnp.where(ranks[b] == j, lengths[b], 0) for b in range(batch_size)]
        ) - device * positions
        living = lax.broadcasted_iota(jnp.int32, (positions, HD), 0) < live
        for h in range(kv_local):
            done = acc_ref[h] / total_ref[h]
            for g in range(per_group):
                n = h * per_group + g
                att_ref[j, :, n * HD:(n + 1) * HD] = jnp.where(
                    living, done[g * positions:(g + 1) * positions], 0.0
                ).astype(jnp.bfloat16)

    def group_sum(j, m, off, side):
        start = (lax.rem(chip + off, chips) * 2 + side) * width
        return jnp.dot(
            att_ref[j, m * STEP_ROWS:(m + 1) * STEP_ROWS, :],
            wo_ref[:, pl.ds(pl.multiple_of(start, width), width)],
            preferred_element_type=jnp.float32,
        ).astype(jnp.bfloat16)

    def pair_copy(i):
        return pltpu.make_async_remote_copy(
            src_ref=pair_out.at[i], dst_ref=pair_in.at[i],
            send_sem=pair_sent.at[i], recv_sem=pair_got.at[i],
            device_id={"tp": partner}, device_id_type=MESH,
        )

    def far_copy(i, off):
        return pltpu.make_async_remote_copy(
            src_ref=far_out.at[off - 1, i], dst_ref=far_in.at[off - 1, i],
            send_sem=far_sent.at[off - 1, i], recv_sem=far_got.at[off - 1, i],
            device_id={"tp": twin(off)}, device_id_type=MESH,
        )

    def mix(j):
        for m in range(mix_steps):
            i = j * mix_steps + m
            for off in range(chips):
                pair_out[i, off] = group_sum(j, m, off, 1 - core)
            pair_copy(i).start()
        for m in range(mix_steps):
            i = j * mix_steps + m
            sums = [group_sum(j, m, off, core).astype(jnp.float32) for off in range(chips)]
            pair_copy(i).wait_recv()
            for off in range(1, chips):
                both = sums[off] + pair_in[i, off].astype(jnp.float32)
                far_out[off - 1, i] = both.astype(jnp.bfloat16)
                far_copy(i, off).start()
            near[i] = sums[0] + pair_in[i, 0].astype(jnp.float32)

    def relay(t):
        j = t // z
        d = lax.rem(t, z)
        c = device - (d + 1) * columns

        @pl.when((d == 0) & (j > 0))
        def _():
            send_own(j)

        for p in range(PIECES):
            arrival(j, c, p).wait_recv()
            each_send(j, c, p, lambda copy: copy.start())

    def take(j, c):
        for p in range(PIECES):
            arrival(j, c, p).wait_recv()
        attend_far(j, c)

    def slot(j, carry):
        used = j < mine

        @pl.when(used)
        def _():
            project_q(j)
            attend_own(j)

        @pl.when((z == 0) & (j + 1 < row_live))
        def _():
            project_kv(j + 1, 0)

        @pl.when(j == 0)
        def _():
            loads[3].wait()

        @pl.when((j == 0) & (z > 0))
        def _():
            relay(0)

        def step(t, carry):
            d = t // columns
            i = lax.rem(t, columns)
            c = (z - d) * columns + column(i)
            ahead = j * z + d

            @pl.when((i == 0) & (d > 0) & (ahead < row_live * z))
            def _():
                relay(ahead)

            @pl.when(used & (i == 0) & (d > 0))
            def _():
                attend_far(j, c)

            @pl.when(used & (i > 0) & ((d > 0) | (column(i) < x)))
            def _():
                take(j, c)

            return carry

        lax.fori_loop(0, (z + 1) * columns, step, 0)

        @pl.when(used)
        def _():
            attend_end(j)
            mix(j)

        return carry

    lax.fori_loop(0, row_live, slot, 0)

    def finish(j, carry):
        for m in range(mix_steps):
            i = j * mix_steps + m
            pair_copy(i).wait_send()
            mixed = near[i]
            for off in range(1, chips):
                far_copy(i, off).wait()
                mixed = mixed + far_in[off - 1, i].astype(jnp.float32)
            mixed_ref[j, m * STEP_ROWS:(m + 1) * STEP_ROWS, :] = mixed.astype(jnp.bfloat16)
        return carry

    lax.fori_loop(0, mine, finish, 0)

    def blank(j, carry):
        mixed_ref[j] = jnp.zeros(mixed_ref.shape[1:], jnp.bfloat16)
        return carry

    lax.fori_loop(mine, slots, blank, 0)
    for b in range(batch_size):
        out_ref[b] = mixed_ref[ranks[b]]

    def drain(j, carry):
        def back(d, carry):
            c = (z - d) * columns + x
            for p in range(PIECES):
                each_send(j, c, p, lambda copy: copy.wait_send())
            return carry

        return lax.fori_loop(0, z + 1, back, carry)

    lax.fori_loop(0, row_live, drain, 0)


def columns_of(devices):
    return 1 << ((devices.bit_length() - 1) // 2)


def layer(
    reach, collective_id,
    inputs, query_weight, key_weight, value_weight, out_weight, chosen, lengths,
):
    batch_size, positions, model_width = inputs.shape
    kv_local = key_weight.shape[1] // HD
    heads_local = query_weight.shape[1] // HD
    per_group = heads_local // kv_local
    devices = lax.axis_size("kv")
    tp = lax.axis_size("tp")
    chips = tp // 2
    columns = columns_of(devices)
    width = out_weight.shape[1] // tp
    steps = batch_size * (positions // STEP_ROWS)
    rows = per_group * positions
    bf16, f32 = jnp.bfloat16, jnp.float32
    vmem = pl.BlockSpec(memory_space=pltpu.VMEM)
    hbm = pl.BlockSpec(memory_space=pl.ANY)
    dma = pltpu.SemaphoreType.DMA
    pair = pltpu.VMEM((steps, chips, STEP_ROWS, width), bf16)
    far = pltpu.VMEM((chips - 1, steps, STEP_ROWS, width), bf16)
    return pl.pallas_call(
        functools.partial(layer_kernel, reach, columns, kv_local, per_group, tp),
        out_shape=jax.ShapeDtypeStruct((batch_size, positions, width), bf16),
        in_specs=[hbm] * 7,
        out_specs=vmem,
        scratch_shapes=[
            pltpu.SMEM(lengths.shape, jnp.int32),
            pltpu.VMEM(chosen.shape, jnp.int32),
            pltpu.VMEM(inputs.shape, bf16),
            pltpu.VMEM(query_weight.shape, bf16),
            pltpu.VMEM((model_width, 2 * kv_local * HD), bf16),
            pltpu.VMEM(out_weight.shape, bf16),
            pltpu.VMEM((batch_size, devices, positions, 2 * kv_local * HD), bf16),
            pltpu.VMEM((kv_local, rows, HD), bf16),
            pltpu.VMEM((kv_local, rows, HD), f32),
            pltpu.VMEM((kv_local, rows, HD), f32),
            pltpu.VMEM((kv_local, rows, HD), f32),
            pltpu.VMEM((batch_size, positions, heads_local * HD), bf16),
            pair, pair, far, far,
            pltpu.VMEM((steps, STEP_ROWS, width), f32),
            pltpu.VMEM((batch_size, positions, width), bf16),
            dma((6 + batch_size,)),
            dma((batch_size, devices // columns, PIECES)),
            dma((batch_size, devices // columns, max(columns - 1, 1), PIECES)),
            dma((batch_size, devices, PIECES)),
            dma((steps,)), dma((steps,)),
            dma((chips - 1, steps)), dma((chips - 1, steps)),
        ],
        compiler_params=pltpu.CompilerParams(
            collective_id=collective_id, has_side_effects=True, vmem_limit_bytes=60 * 2**20
        ),
    )(lengths, inputs, query_weight, key_weight, value_weight, out_weight, chosen)


def fits_kernel(limits, length_ref, out_ref):
    lengths = [length_ref[b] for b in range(length_ref.shape[0])]
    fits = jnp.int32(1)
    for j, limit in enumerate(limits):
        longer = sum([(length > limit).astype(jnp.int32) for length in lengths])
        fits = fits * (longer <= j).astype(jnp.int32)
    out_ref[0] = fits


def fits_short(lengths, limits):
    smem = pl.BlockSpec(memory_space=pltpu.SMEM)
    return pl.pallas_call(
        functools.partial(fits_kernel, limits),
        out_shape=jax.ShapeDtypeStruct((1,), jnp.int32),
        in_specs=[smem], out_specs=smem,
    )(lengths)


def shards(*args):
    inputs, lengths = args[0], args[-1]
    batch_size, positions, _ = inputs.shape
    short, whole = spans(batch_size, lax.axis_size("kv"), positions)
    fits = fits_short(lengths, tuple(span * positions for span in short))
    return lax.cond(
        fits[0] > 0,
        functools.partial(layer, short, 0),
        functools.partial(layer, whole, 1),
        *args,
    )


def solution(mesh):
    placed = (
        P(None, "kv", None),
        P(None, "tp"),
        P(None, "tp"),
        P(None, "tp"),
        P("tp", None),
        P(None, "kv", None),
        P(),
    )
    return jax.shard_map(
        shards, mesh=mesh, in_specs=placed, out_specs=P(None, "kv", "tp"), check_vma=False
    )
```

```python
import functools

import jax
import jax.numpy as jnp
from jax import lax
from jax.experimental import pallas as pl
from jax.experimental.pallas import tpu as pltpu
from jax.sharding import PartitionSpec as P

HD = 128
KB = 64
MASKED = -1e30
PIECES = 2
STEP_ROWS = 128
MESH = pl.DeviceIdType.MESH


def spans(batch_size, devices, positions):
    seq = devices * positions
    total = seq + seq // 2
    longest = [min(seq, (total - (batch_size - 1 - j)) // (j + 1)) for j in range(batch_size)]
    whole = tuple(-(-length // positions) for length in longest)
    short = tuple(
        min(full, -(-devices * 3 // (8 * j)) if j else devices) for j, full in enumerate(whole)
    )
    return short, whole


def layer_kernel(
    reach, columns, kv_local, per_group, tp,
    length_hbm, x_hbm, wq_hbm, wk_hbm, wv_hbm, wo_hbm, chosen_hbm, out_ref,
    length_ref, chosen_ref, x_ref, wq_ref, wkv_ref, wo_ref, kv_ref, q_ref,
    top_ref, total_ref, acc_ref, att_ref,
    pair_out, pair_in, far_out, far_in, near, mixed_ref,
    load_sem, z_sent, x_sent, aside, got, pair_sent, pair_got, far_sent, far_got,
):
    batch_size, positions, _ = x_ref.shape
    slots, devices = kv_ref.shape[:2]
    rows_z = devices // columns
    per_dev = positions // KB
    half = kv_local * HD
    rows = per_group * positions
    width = out_ref.shape[-1]
    piece_rows = positions // PIECES
    mix_steps = positions // STEP_ROWS
    scaling = HD ** (-0.5)
    contract = (((1,), (1,)), ((), ()))

    device = lax.axis_index("kv")
    z = device // columns
    x = lax.rem(device, columns)
    me = lax.axis_index("tp")
    core = lax.rem(me, 2)
    chip = me // 2
    chips = tp // 2
    partner = me + 1 - 2 * core

    def live_at(r):
        return sum([(r < reach[j]).astype(jnp.int32) for j in range(slots)])

    def column(i):
        return lax.rem(x + i, columns)

    def twin(off):
        return lax.rem(chip + off, chips) * 2 + core

    mine = live_at(device)
    row_live = live_at(z * columns)
    next_live = live_at((z + 1) * columns)

    loads = [
        pltpu.make_async_copy(wk_hbm, wkv_ref.at[:, pl.ds(0, half)], load_sem.at[0]),
        pltpu.make_async_copy(wv_hbm, wkv_ref.at[:, pl.ds(half, half)], load_sem.at[1]),
        pltpu.make_async_copy(wq_hbm, wq_ref, load_sem.at[2]),
        pltpu.make_async_copy(wo_hbm, wo_ref, load_sem.at[3]),
        pltpu.make_async_copy(length_hbm, length_ref, load_sem.at[4]),
        pltpu.make_async_copy(chosen_hbm, chosen_ref, load_sem.at[5]),
        pltpu.make_async_copy(x_hbm, x_ref, load_sem.at[6]),
    ]
    loads[4].start()
    loads[6].start()
    loads[0].start()
    loads[1].start()
    loads[5].start()

    barrier = pltpu.get_barrier_semaphore()

    def greet(**where):
        pl.semaphore_signal(barrier, inc=1, device_id=where, device_id_type=MESH)

    greet(tp=partner)
    for off in range(1, chips):
        greet(tp=twin(off))
    for i in range(1, columns):
        greet(kv=z * columns + column(i))

    @pl.when(z > 0)
    def _():
        greet(kv=device - columns)

    @pl.when(z < rows_z - 1)
    def _():
        greet(kv=device + columns)

    loads[4].wait()
    lengths = [length_ref[b] for b in range(batch_size)]
    ranks = []
    for b in range(batch_size):
        ahead = [
            (lengths[o] >= lengths[b] if o < b else lengths[o] > lengths[b]).astype(jnp.int32)
            for o in range(batch_size) if o != b
        ]
        ranks.append(sum(ahead))

    def holder(j):
        return sum([jnp.where(ranks[b] == j, b, 0) for b in range(batch_size)])

    def at_slot(j, row):
        return row + sum(
            [jnp.where(k < j, -(-reach[k] // columns), 0) for k in range(slots - 1)]
        )

    def part(j, c, p, n):
        return kv_ref.at[j, c, pl.ds(p * piece_rows, n * piece_rows)]

    def send(j, c, p, n, sent, where):
        return pltpu.make_async_remote_copy(
            src_ref=part(j, c, p, n), dst_ref=part(j, c, p, n), send_sem=sent,
            recv_sem=got.at[at_slot(j, c // columns), lax.rem(c, columns), p],
            device_id=where, device_id_type=MESH,
        )

    def z_copy(j, c, p, n=1):
        return send(
            j, c, p, n, z_sent.at[at_slot(j, c // columns)], {"kv": device + columns}
        )

    def x_copy(j, c, p, i, n=1):
        return send(
            j, c, p, n, x_sent.at[at_slot(j, c // columns), i - 1],
            {"kv": z * columns + column(i)},
        )

    def aside_copy(j):
        first = PIECES // 2
        return send(j, device - 1, first, PIECES - first, aside.at[j], {"kv": device + columns})

    def arrival(j, c, p):
        return send(j, c, p, 1, z_sent.at[at_slot(j, c // columns)], {"tp": partner})

    def by_z(c, i):
        return (c == device - columns) & (x == 0) & (column(i) == 1)

    def to_row(j, c, i):
        own = c == device
        return (j < live_at(z * columns + column(i))) & (
            jnp.logical_not(own) | (column(i) > x)
        )

    def each_send(j, c, p):
        @pl.when(j < next_live)
        def _():
            z_copy(j, c, p).start()

        for i in range(1, columns):
            wanted = to_row(j, c, i)
            if p >= PIECES // 2:
                wanted = wanted & jnp.logical_not(by_z(c, i))

            @pl.when(wanted)
            def _():
                x_copy(j, c, p, i).start()

    def each_sent(j, c):
        @pl.when(j < next_live)
        def _():
            z_copy(j, c, 0, PIECES).wait_send()

        for i in range(1, columns):
            @pl.when(to_row(j, c, i) & by_z(c, i))
            def _():
                x_copy(j, c, 0, i, PIECES // 2).wait_send()

            @pl.when(to_row(j, c, i) & jnp.logical_not(by_z(c, i)))
            def _():
                x_copy(j, c, 0, i, PIECES).wait_send()

    def put_aside(j, act):
        @pl.when((x == 1) & (j < live_at(device + columns)))
        def _():
            act(aside_copy(j))

    def send_own(j):
        for p in range(PIECES):
            each_send(j, device, p)

    loads[0].wait()
    loads[1].wait()
    loads[6].wait()

    loads[2].start()

    def project_kv(j, carry):
        kv_ref[j, device] = jnp.dot(
            x_ref[holder(j)], wkv_ref[...], preferred_element_type=jnp.float32
        ).astype(jnp.bfloat16)

        @pl.when(j == 0)
        def _():
            pl.semaphore_wait(
                barrier,
                chips + columns - 1
                + (z > 0).astype(jnp.int32) + (z < rows_z - 1).astype(jnp.int32),
            )

        @pl.when((j == 0) | (z == 0))
        def _():
            send_own(j)

        return carry

    lax.fori_loop(0, jnp.where(z == 0, 1, row_live), project_kv, 0)
    loads[3].start()
    loads[2].wait()
    loads[5].wait()

    def project_q(j):
        queries = jnp.dot(
            x_ref[holder(j)], wq_ref[...], preferred_element_type=jnp.float32
        ).astype(jnp.bfloat16)
        for n in range(kv_local * per_group):
            h, g = n // per_group, n % per_group
            q_ref[h, g * positions:(g + 1) * positions, :] = queries[:, n * HD:(n + 1) * HD]

    def named(names, c):
        segment = lax.broadcasted_iota(jnp.int32, (per_dev, positions), 1) // KB
        bias = jnp.full((per_dev, positions), MASKED, jnp.float32)
        for i in range(per_dev):
            hit = jnp.max(
                jnp.where(names == c * per_dev + i, 0.0, MASKED), axis=1, keepdims=True
            )
            bias = jnp.where(segment == i, hit, bias)
        return jnp.broadcast_to(bias[:, None, :], (per_dev, KB, positions)).reshape(
            positions, positions
        )

    def scores(j, c, h, bias):
        raw = lax.dot_general(
            q_ref[h], kv_ref[j, c, :, h * HD:(h + 1) * HD], contract,
            preferred_element_type=jnp.float32,
        )
        shaped = (raw * scaling).reshape(per_group, positions, positions) + bias[None]
        return shaped.reshape(rows, positions)

    def weigh(j, c, h, raised):
        return jnp.dot(
            raised.astype(jnp.bfloat16), kv_ref[j, c, :, half + h * HD:half + (h + 1) * HD],
            preferred_element_type=jnp.float32,
        )

    def wide(value):
        return jnp.concatenate([value] * (positions // HD), axis=1)

    def attend_own(j):
        names = chosen_ref[holder(j)]
        before = named(names, device)
        home = device * per_dev + lax.broadcasted_iota(jnp.int32, names.shape, 0)
        copies = jnp.sum(jnp.where(names == home, 1.0, 0.0), axis=1, keepdims=True)
        same = jnp.log(jnp.maximum(copies, 1.0))
        same = jnp.broadcast_to(same[:, None, :], (per_dev, KB, positions)).reshape(
            positions, positions
        )
        at_row = lax.broadcasted_iota(jnp.int32, (positions, positions), 0)
        at_col = lax.broadcasted_iota(jnp.int32, (positions, positions), 1)
        bias = jnp.where(at_col < at_row, before, jnp.where(at_col == at_row, same, MASKED))
        for h in range(kv_local):
            s = scores(j, device, h, bias)
            top = jnp.broadcast_to(jnp.max(s, axis=1, keepdims=True), (rows, HD))
            raised = jnp.exp(s - wide(top))
            top_ref[h] = top
            total_ref[h] = jnp.broadcast_to(jnp.sum(raised, axis=1, keepdims=True), (rows, HD))
            acc_ref[h] = weigh(j, device, h, raised)

    def attend_far(j, c):
        bias = named(chosen_ref[holder(j)], c)
        for h in range(kv_local):
            s = scores(j, c, h, bias)
            old = top_ref[h]
            top = jnp.maximum(old, jnp.max(s, axis=1, keepdims=True))
            fade = jnp.exp(old - top)
            raised = jnp.exp(s - wide(top))
            top_ref[h] = top
            total_ref[h] = total_ref[h] * fade + jnp.sum(raised, axis=1, keepdims=True)
            acc_ref[h] = acc_ref[h] * fade + weigh(j, c, h, raised)

    def attend_end(j):
        live = sum(
            [jnp.where(ranks[b] == j, lengths[b], 0) for b in range(batch_size)]
        ) - device * positions
        living = lax.broadcasted_iota(jnp.int32, (positions, HD), 0) < live
        for h in range(kv_local):
            done = acc_ref[h] / total_ref[h]
            for g in range(per_group):
                n = h * per_group + g
                att_ref[j, :, n * HD:(n + 1) * HD] = jnp.where(
                    living, done[g * positions:(g + 1) * positions], 0.0
                ).astype(jnp.bfloat16)

    def group_sum(j, m, off, side):
        start = (lax.rem(chip + off, chips) * 2 + side) * width
        return jnp.dot(
            att_ref[j, m * STEP_ROWS:(m + 1) * STEP_ROWS, :],
            wo_ref[:, pl.ds(pl.multiple_of(start, width), width)],
            preferred_element_type=jnp.float32,
        ).astype(jnp.bfloat16)

    def pair_copy(i):
        return pltpu.make_async_remote_copy(
            src_ref=pair_out.at[i], dst_ref=pair_in.at[i],
            send_sem=pair_sent.at[i], recv_sem=pair_got.at[lax.rem(i, 2 * mix_steps)],
            device_id={"tp": partner}, device_id_type=MESH,
        )

    def far_copy(i, off):
        return pltpu.make_async_remote_copy(
            src_ref=far_out.at[off - 1, i], dst_ref=far_in.at[off - 1, i],
            send_sem=far_sent.at[off - 1, i], recv_sem=far_got.at[off - 1, i],
            device_id={"tp": twin(off)}, device_id_type=MESH,
        )

    def mix(j):
        for m in range(mix_steps):
            i = j * mix_steps + m
            for off in range(chips):
                pair_out[i, off] = group_sum(j, m, off, 1 - core)
            pair_copy(i).start()
        for m in range(mix_steps):
            i = j * mix_steps + m
            sums = [group_sum(j, m, off, core).astype(jnp.float32) for off in range(chips)]
            pair_copy(i).wait_recv()
            for off in range(1, chips):
                both = sums[off] + pair_in[i, off].astype(jnp.float32)
                far_out[off - 1, i] = both.astype(jnp.bfloat16)
                far_copy(i, off).start()
            near[i] = sums[0] + pair_in[i, 0].astype(jnp.float32)

    def relay(t):
        j = t // z
        d = lax.rem(t, z)
        c = device - (d + 1) * columns

        @pl.when((d == 0) & (j > 0))
        def _():
            send_own(j)

        for p in range(PIECES):
            arrival(j, c, p).wait_recv()
            each_send(j, c, p)

    def take(j, c):
        for p in range(PIECES):
            arrival(j, c, p).wait_recv()
        attend_far(j, c)

    def slot(j, carry):
        used = j < mine

        @pl.when(used)
        def _():
            project_q(j)
            attend_own(j)

        @pl.when((z == 0) & (j + 1 < row_live))
        def _():
            project_kv(j + 1, 0)

        @pl.when(j == 0)
        def _():
            loads[3].wait()

        @pl.when((j == 0) & (z > 0))
        def _():
            relay(0)

        def step(t, carry):
            d = t // columns
            i = lax.rem(t, columns)
            ahead = j * z + d
            below = (i == 0) & (d > 0) & (d <= z)

            @pl.when((z > 0) & (i == 0) & (d == jnp.maximum(z, 2)))
            def _():
                put_aside(j, lambda copy: copy.start())

            @pl.when(below & (ahead < row_live * z))
            def _():
                relay(ahead)

            @pl.when(used & below)
            def _():
                attend_far(j, device - d * columns)

            other = column(i)
            late = (x == 1) & (other == 0)
            last = d - 1
            back = jnp.where(late & (last > 0), lax.rem(last, jnp.maximum(z, 1)) + 1, last)

            @pl.when(used & (i > 0) & (d > 0) & ((last > 0) | (other < x)))
            def _():
                take(j, (z - back) * columns + other)

            return carry

        lax.fori_loop(0, (z + 2) * columns, step, 0)

        @pl.when(z == 0)
        def _():
            put_aside(j, lambda copy: copy.start())

        @pl.when(used)
        def _():
            attend_end(j)
            mix(j)

        return carry

    lax.fori_loop(0, row_live, slot, 0)

    def finish(j, carry):
        for m in range(mix_steps):
            i = j * mix_steps + m
            pair_copy(i).wait_send()
            mixed = near[i]
            for off in range(1, chips):
                far_copy(i, off).wait()
                mixed = mixed + far_in[off - 1, i].astype(jnp.float32)
            mixed_ref[j, m * STEP_ROWS:(m + 1) * STEP_ROWS, :] = mixed.astype(jnp.bfloat16)
        return carry

    lax.fori_loop(0, mine, finish, 0)

    def blank(j, carry):
        mixed_ref[j] = jnp.zeros(mixed_ref.shape[1:], jnp.bfloat16)
        return carry

    lax.fori_loop(mine, slots, blank, 0)
    for b in range(batch_size):
        out_ref[b] = mixed_ref[ranks[b]]

    def drain(j, carry):
        def back(d, carry):
            c = (z - d) * columns + x
            each_sent(j, c)
            return carry

        put_aside(j, lambda copy: copy.wait_send())
        return lax.fori_loop(0, z + 1, back, carry)

    lax.fori_loop(0, row_live, drain, 0)


def columns_of(devices):
    return 1 << ((devices.bit_length() - 1) // 2)


def layer(
    reach, collective_id,
    inputs, query_weight, key_weight, value_weight, out_weight, chosen, lengths,
):
    batch_size, positions, model_width = inputs.shape
    kv_local = key_weight.shape[1] // HD
    heads_local = query_weight.shape[1] // HD
    per_group = heads_local // kv_local
    devices = lax.axis_size("kv")
    tp = lax.axis_size("tp")
    chips = tp // 2
    columns = columns_of(devices)
    width = out_weight.shape[1] // tp
    steps = batch_size * (positions // STEP_ROWS)
    rows = per_group * positions
    reached = sum([-(-span // columns) for span in reach])
    bf16, f32 = jnp.bfloat16, jnp.float32
    vmem = pl.BlockSpec(memory_space=pltpu.VMEM)
    hbm = pl.BlockSpec(memory_space=pl.ANY)
    dma = pltpu.SemaphoreType.DMA
    pair = pltpu.VMEM((steps, chips, STEP_ROWS, width), bf16)
    far = pltpu.VMEM((chips - 1, steps, STEP_ROWS, width), bf16)
    return pl.pallas_call(
        functools.partial(layer_kernel, reach, columns, kv_local, per_group, tp),
        out_shape=jax.ShapeDtypeStruct((batch_size, positions, width), bf16),
        in_specs=[hbm] * 7,
        out_specs=vmem,
        scratch_shapes=[
            pltpu.SMEM(lengths.shape, jnp.int32),
            pltpu.VMEM(chosen.shape, jnp.int32),
            pltpu.VMEM(inputs.shape, bf16),
            pltpu.VMEM(query_weight.shape, bf16),
            pltpu.VMEM((model_width, 2 * kv_local * HD), bf16),
            pltpu.VMEM(out_weight.shape, bf16),
            pltpu.VMEM((batch_size, devices, positions, 2 * kv_local * HD), bf16),
            pltpu.VMEM((kv_local, rows, HD), bf16),
            pltpu.VMEM((kv_local, rows, HD), f32),
            pltpu.VMEM((kv_local, rows, HD), f32),
            pltpu.VMEM((kv_local, rows, HD), f32),
            pltpu.VMEM((batch_size, positions, heads_local * HD), bf16),
            pair, pair, far, far,
            pltpu.VMEM((steps, STEP_ROWS, width), f32),
            pltpu.VMEM((batch_size, positions, width), bf16),
            dma((7,)),
            dma((reached,)),
            dma((reached, max(columns - 1, 1))),
            dma((batch_size,)),
            dma((reached, columns, PIECES)),
            dma((steps,)), dma((2 * (positions // STEP_ROWS),)),
            dma((chips - 1, steps)), dma((chips - 1, steps)),
        ],
        compiler_params=pltpu.CompilerParams(
            collective_id=collective_id, has_side_effects=True, vmem_limit_bytes=60 * 2**20
        ),
    )(lengths, inputs, query_weight, key_weight, value_weight, out_weight, chosen)


def fits_kernel(limits, length_ref, out_ref):
    lengths = [length_ref[b] for b in range(length_ref.shape[0])]
    fits = jnp.int32(1)
    for j, limit in enumerate(limits):
        longer = sum([(length > limit).astype(jnp.int32) for length in lengths])
        fits = fits * (longer <= j).astype(jnp.int32)
    out_ref[0] = fits


def fits_short(lengths, limits):
    smem = pl.BlockSpec(memory_space=pltpu.SMEM)
    return pl.pallas_call(
        functools.partial(fits_kernel, limits),
        out_shape=jax.ShapeDtypeStruct((1,), jnp.int32),
        in_specs=[smem], out_specs=smem,
    )(lengths)


def shards(*args):
    inputs, lengths = args[0], args[-1]
    batch_size, positions, _ = inputs.shape
    short, whole = spans(batch_size, lax.axis_size("kv"), positions)
    fits = fits_short(lengths, tuple(span * positions for span in short))
    return lax.cond(
        fits[0] > 0,
        functools.partial(layer, short, 0),
        functools.partial(layer, whole, 1),
        *args,
    )


def solution(mesh):
    placed = (
        P(None, "kv", None),
        P(None, "tp"),
        P(None, "tp"),
        P(None, "tp"),
        P("tp", None),
        P(None, "kv", None),
        P(),
    )
    return jax.shard_map(
        shards, mesh=mesh, in_specs=placed, out_specs=P(None, "kv", "tp"), check_vma=False
    )
```

```python
import functools

import jax
import jax.numpy as jnp
from jax import lax
from jax.experimental import pallas as pl
from jax.experimental.pallas import tpu as pltpu
from jax.sharding import PartitionSpec as P

HD = 128
KB = 64
MASKED = -1e30
PIECES = 2
STEP_ROWS = 128
MESH = pl.DeviceIdType.MESH


def spans(batch_size, devices, positions):
    seq = devices * positions
    total = seq + seq // 2
    longest = [min(seq, (total - (batch_size - 1 - j)) // (j + 1)) for j in range(batch_size)]
    whole = tuple(-(-length // positions) for length in longest)
    short = tuple(
        min(full, -(-devices * 3 // (8 * j)) if j else devices) for j, full in enumerate(whole)
    )
    return short, whole


def layer_kernel(
    reach, columns, kv_local, per_group, tp,
    slot_ref, x_ref, wkv_ref, wq_hbm, wo_hbm, chosen_hbm, out_ref,
    chosen_ref, wq_ref, wo_ref, kv_ref, q_ref,
    top_ref, total_ref, acc_ref, att_ref,
    pair_out, pair_in, far_out, far_in, near, mixed_ref,
    load_sem, z_sent, x_sent, aside, got, pair_sent, pair_got, far_sent, far_got,
):
    batch_size, positions, _ = x_ref.shape
    slots, devices = kv_ref.shape[:2]
    rows_z = devices // columns
    per_dev = positions // KB
    half = kv_local * HD
    rows = per_group * positions
    width = out_ref.shape[-1]
    piece_rows = positions // PIECES
    mix_steps = positions // STEP_ROWS
    scaling = HD ** (-0.5)
    contract = (((1,), (1,)), ((), ()))

    device = lax.axis_index("kv")
    z = device // columns
    x = lax.rem(device, columns)
    me = lax.axis_index("tp")
    core = lax.rem(me, 2)
    chip = me // 2
    chips = tp // 2
    partner = me + 1 - 2 * core

    def live_at(r):
        return sum([(r < reach[j]).astype(jnp.int32) for j in range(slots)])

    def column(i):
        return lax.rem(x + i, columns)

    def twin(off):
        return lax.rem(chip + off, chips) * 2 + core

    mine = live_at(device)
    row_live = live_at(z * columns)
    next_live = live_at((z + 1) * columns)

    loads = [
        pltpu.make_async_copy(wq_hbm, wq_ref, load_sem.at[0]),
        pltpu.make_async_copy(chosen_hbm, chosen_ref, load_sem.at[1]),
        pltpu.make_async_copy(wo_hbm, wo_ref, load_sem.at[2]),
    ]
    for load in loads:
        load.start()

    barrier = pltpu.get_barrier_semaphore()

    def greet(**where):
        pl.semaphore_signal(barrier, inc=1, device_id=where, device_id_type=MESH)

    greet(tp=partner)
    for off in range(1, chips):
        greet(tp=twin(off))
    for i in range(1, columns):
        greet(kv=z * columns + column(i))

    @pl.when(z > 0)
    def _():
        greet(kv=device - columns)

    @pl.when(z < rows_z - 1)
    def _():
        greet(kv=device + columns)

    def holder(j):
        return slot_ref[1 + j]

    def at_slot(j, row):
        return row + sum(
            [jnp.where(k < j, -(-reach[k] // columns), 0) for k in range(slots - 1)]
        )

    def part(j, c, p, n):
        return kv_ref.at[j, c, pl.ds(p * piece_rows, n * piece_rows)]

    def send(j, c, p, n, sent, where):
        return pltpu.make_async_remote_copy(
            src_ref=part(j, c, p, n), dst_ref=part(j, c, p, n), send_sem=sent,
            recv_sem=got.at[at_slot(j, c // columns), lax.rem(c, columns), p],
            device_id=where, device_id_type=MESH,
        )

    def z_copy(j, c, p, n=1):
        return send(
            j, c, p, n, z_sent.at[at_slot(j, c // columns)], {"kv": device + columns}
        )

    def x_copy(j, c, p, i, n=1):
        return send(
            j, c, p, n, x_sent.at[at_slot(j, c // columns), i - 1],
            {"kv": z * columns + column(i)},
        )

    def aside_copy(j):
        first = PIECES // 2
        return send(j, device - 1, first, PIECES - first, aside.at[j], {"kv": device + columns})

    def arrival(j, c, p):
        return send(j, c, p, 1, z_sent.at[at_slot(j, c // columns)], {"tp": partner})

    def by_z(c, i):
        return (c == device - columns) & (x == 0) & (column(i) == 1)

    def to_row(j, c, i):
        own = c == device
        return (j < live_at(z * columns + column(i))) & (
            jnp.logical_not(own) | (column(i) > x)
        )

    def each_send(j, c, p):
        @pl.when(j < next_live)
        def _():
            z_copy(j, c, p).start()

        for i in range(1, columns):
            wanted = to_row(j, c, i)
            if p >= PIECES // 2:
                wanted = wanted & jnp.logical_not(by_z(c, i))

            @pl.when(wanted)
            def _():
                x_copy(j, c, p, i).start()

    def each_sent(j, c):
        @pl.when(j < next_live)
        def _():
            z_copy(j, c, 0, PIECES).wait_send()

        for i in range(1, columns):
            @pl.when(to_row(j, c, i) & by_z(c, i))
            def _():
                x_copy(j, c, 0, i, PIECES // 2).wait_send()

            @pl.when(to_row(j, c, i) & jnp.logical_not(by_z(c, i)))
            def _():
                x_copy(j, c, 0, i, PIECES).wait_send()

    def put_aside(j, act):
        @pl.when((x == 1) & (j < live_at(device + columns)))
        def _():
            act(aside_copy(j))

    def send_own(j):
        for p in range(PIECES):
            each_send(j, device, p)

    def project_kv(j, carry):
        kv_ref[j, device] = jnp.dot(
            x_ref[j], wkv_ref[...], preferred_element_type=jnp.float32
        ).astype(jnp.bfloat16)

        @pl.when(j == 0)
        def _():
            pl.semaphore_wait(
                barrier,
                chips + columns - 1
                + (z > 0).astype(jnp.int32) + (z < rows_z - 1).astype(jnp.int32),
            )

        @pl.when((j == 0) | (z == 0))
        def _():
            send_own(j)

        return carry

    lax.fori_loop(0, jnp.where(z == 0, 1, row_live), project_kv, 0)
    loads[0].wait()
    loads[1].wait()

    def project_q(j):
        queries = jnp.dot(
            x_ref[j], wq_ref[...], preferred_element_type=jnp.float32
        ).astype(jnp.bfloat16)
        for n in range(kv_local * per_group):
            h, g = n // per_group, n % per_group
            q_ref[h, g * positions:(g + 1) * positions, :] = queries[:, n * HD:(n + 1) * HD]

    def named(names, c):
        segment = lax.broadcasted_iota(jnp.int32, (per_dev, positions), 1) // KB
        bias = jnp.full((per_dev, positions), MASKED, jnp.float32)
        for i in range(per_dev):
            hit = jnp.max(
                jnp.where(names == c * per_dev + i, 0.0, MASKED), axis=1, keepdims=True
            )
            bias = jnp.where(segment == i, hit, bias)
        return jnp.broadcast_to(bias[:, None, :], (per_dev, KB, positions)).reshape(
            positions, positions
        )

    def scores(j, c, h, bias):
        raw = lax.dot_general(
            q_ref[h], kv_ref[j, c, :, h * HD:(h + 1) * HD], contract,
            preferred_element_type=jnp.float32,
        )
        shaped = (raw * scaling).reshape(per_group, positions, positions) + bias[None]
        return shaped.reshape(rows, positions)

    def weigh(j, c, h, raised):
        return jnp.dot(
            raised.astype(jnp.bfloat16), kv_ref[j, c, :, half + h * HD:half + (h + 1) * HD],
            preferred_element_type=jnp.float32,
        )

    def wide(value):
        return jnp.concatenate([value] * (positions // HD), axis=1)

    def attend_own(j):
        names = chosen_ref[holder(j)]
        before = named(names, device)
        home = device * per_dev + lax.broadcasted_iota(jnp.int32, names.shape, 0)
        copies = jnp.sum(jnp.where(names == home, 1.0, 0.0), axis=1, keepdims=True)
        same = jnp.log(jnp.maximum(copies, 1.0))
        same = jnp.broadcast_to(same[:, None, :], (per_dev, KB, positions)).reshape(
            positions, positions
        )
        at_row = lax.broadcasted_iota(jnp.int32, (positions, positions), 0)
        at_col = lax.broadcasted_iota(jnp.int32, (positions, positions), 1)
        bias = jnp.where(at_col < at_row, before, jnp.where(at_col == at_row, same, MASKED))
        for h in range(kv_local):
            s = scores(j, device, h, bias)
            top = jnp.broadcast_to(jnp.max(s, axis=1, keepdims=True), (rows, HD))
            raised = jnp.exp(s - wide(top))
            top_ref[h] = top
            total_ref[h] = jnp.broadcast_to(jnp.sum(raised, axis=1, keepdims=True), (rows, HD))
            acc_ref[h] = weigh(j, device, h, raised)

    def attend_far(j, c):
        bias = named(chosen_ref[holder(j)], c)
        for h in range(kv_local):
            s = scores(j, c, h, bias)
            old = top_ref[h]
            top = jnp.maximum(old, jnp.max(s, axis=1, keepdims=True))
            fade = jnp.exp(old - top)
            raised = jnp.exp(s - wide(top))
            top_ref[h] = top
            total_ref[h] = total_ref[h] * fade + jnp.sum(raised, axis=1, keepdims=True)
            acc_ref[h] = acc_ref[h] * fade + weigh(j, c, h, raised)

    def attend_end(j):
        live = slot_ref[1 + 2 * batch_size + j] - device * positions
        living = lax.broadcasted_iota(jnp.int32, (positions, HD), 0) < live
        for h in range(kv_local):
            done = acc_ref[h] / total_ref[h]
            for g in range(per_group):
                n = h * per_group + g
                att_ref[j, :, n * HD:(n + 1) * HD] = jnp.where(
                    living, done[g * positions:(g + 1) * positions], 0.0
                ).astype(jnp.bfloat16)

    def group_sum(j, m, off, side):
        start = (lax.rem(chip + off, chips) * 2 + side) * width
        return jnp.dot(
            att_ref[j, m * STEP_ROWS:(m + 1) * STEP_ROWS, :],
            wo_ref[:, pl.ds(pl.multiple_of(start, width), width)],
            preferred_element_type=jnp.float32,
        ).astype(jnp.bfloat16)

    def pair_copy(i):
        return pltpu.make_async_remote_copy(
            src_ref=pair_out.at[i], dst_ref=pair_in.at[i],
            send_sem=pair_sent.at[i], recv_sem=pair_got.at[lax.rem(i, 2 * mix_steps)],
            device_id={"tp": partner}, device_id_type=MESH,
        )

    def far_copy(i, off):
        return pltpu.make_async_remote_copy(
            src_ref=far_out.at[off - 1, i], dst_ref=far_in.at[off - 1, i],
            send_sem=far_sent.at[off - 1, i], recv_sem=far_got.at[off - 1, i],
            device_id={"tp": twin(off)}, device_id_type=MESH,
        )

    def mix(j):
        for m in range(mix_steps):
            i = j * mix_steps + m
            for off in range(chips):
                pair_out[i, off] = group_sum(j, m, off, 1 - core)
            pair_copy(i).start()
        for m in range(mix_steps):
            i = j * mix_steps + m
            sums = [group_sum(j, m, off, core).astype(jnp.float32) for off in range(chips)]
            pair_copy(i).wait_recv()
            for off in range(1, chips):
                both = sums[off] + pair_in[i, off].astype(jnp.float32)
                far_out[off - 1, i] = both.astype(jnp.bfloat16)
                far_copy(i, off).start()
            near[i] = sums[0] + pair_in[i, 0].astype(jnp.float32)

    def relay(t):
        j = t // z
        d = lax.rem(t, z)
        c = device - (d + 1) * columns

        @pl.when((d == 0) & (j > 0))
        def _():
            send_own(j)

        for p in range(PIECES):
            arrival(j, c, p).wait_recv()
            each_send(j, c, p)

    def take(j, c):
        for p in range(PIECES):
            arrival(j, c, p).wait_recv()
        attend_far(j, c)

    def slot(j, carry):
        used = j < mine

        @pl.when(used)
        def _():
            project_q(j)
            attend_own(j)

        @pl.when((z == 0) & (j + 1 < row_live))
        def _():
            project_kv(j + 1, 0)

        @pl.when(j == 0)
        def _():
            loads[2].wait()

        @pl.when((j == 0) & (z > 0))
        def _():
            relay(0)

        def step(t, carry):
            d = t // columns
            i = lax.rem(t, columns)
            ahead = j * z + d
            below = (i == 0) & (d > 0) & (d <= z)

            @pl.when((z > 0) & (i == 0) & (d == jnp.maximum(z, 2)))
            def _():
                put_aside(j, lambda copy: copy.start())

            @pl.when(below & (ahead < row_live * z))
            def _():
                relay(ahead)

            @pl.when(used & below)
            def _():
                attend_far(j, device - d * columns)

            other = column(i)
            late = (x == 1) & (other == 0)
            last = d - 1
            back = jnp.where(late & (last > 0), lax.rem(last, jnp.maximum(z, 1)) + 1, last)

            @pl.when(used & (i > 0) & (d > 0) & ((last > 0) | (other < x)))
            def _():
                take(j, (z - back) * columns + other)

            return carry

        lax.fori_loop(0, (z + 2) * columns, step, 0)

        @pl.when(z == 0)
        def _():
            put_aside(j, lambda copy: copy.start())

        @pl.when(used)
        def _():
            attend_end(j)
            mix(j)

        return carry

    lax.fori_loop(0, row_live, slot, 0)

    def finish(j, carry):
        for m in range(mix_steps):
            i = j * mix_steps + m
            pair_copy(i).wait_send()
            mixed = near[i]
            for off in range(1, chips):
                far_copy(i, off).wait()
                mixed = mixed + far_in[off - 1, i].astype(jnp.float32)
            mixed_ref[j, m * STEP_ROWS:(m + 1) * STEP_ROWS, :] = mixed.astype(jnp.bfloat16)
        return carry

    lax.fori_loop(0, mine, finish, 0)

    def blank(j, carry):
        mixed_ref[j] = jnp.zeros(mixed_ref.shape[1:], jnp.bfloat16)
        return carry

    lax.fori_loop(mine, slots, blank, 0)
    for b in range(batch_size):
        out_ref[b] = mixed_ref[slot_ref[1 + batch_size + b]]

    def drain(j, carry):
        def back(d, carry):
            c = (z - d) * columns + x
            each_sent(j, c)
            return carry

        put_aside(j, lambda copy: copy.wait_send())
        return lax.fori_loop(0, z + 1, back, carry)

    lax.fori_loop(0, row_live, drain, 0)


def columns_of(devices):
    return 1 << ((devices.bit_length() - 1) // 2)


def layer(
    reach, collective_id, slot, x, key_value_weight,
    query_weight, out_weight, chosen,
):
    batch_size, positions, _ = x.shape
    kv_local = key_value_weight.shape[1] // (2 * HD)
    heads_local = query_weight.shape[1] // HD
    per_group = heads_local // kv_local
    devices = lax.axis_size("kv")
    tp = lax.axis_size("tp")
    chips = tp // 2
    columns = columns_of(devices)
    width = out_weight.shape[1] // tp
    steps = batch_size * (positions // STEP_ROWS)
    rows = per_group * positions
    reached = sum([-(-span // columns) for span in reach])
    bf16, f32 = jnp.bfloat16, jnp.float32
    vmem = pl.BlockSpec(memory_space=pltpu.VMEM)
    smem = pl.BlockSpec(memory_space=pltpu.SMEM)
    hbm = pl.BlockSpec(memory_space=pl.ANY)
    dma = pltpu.SemaphoreType.DMA
    pair = pltpu.VMEM((steps, chips, STEP_ROWS, width), bf16)
    far = pltpu.VMEM((chips - 1, steps, STEP_ROWS, width), bf16)
    return pl.pallas_call(
        functools.partial(layer_kernel, reach, columns, kv_local, per_group, tp),
        out_shape=jax.ShapeDtypeStruct((batch_size, positions, width), bf16),
        in_specs=[smem, vmem, vmem, hbm, hbm, hbm],
        out_specs=vmem,
        scratch_shapes=[
            pltpu.VMEM(chosen.shape, jnp.int32),
            pltpu.VMEM(query_weight.shape, bf16),
            pltpu.VMEM(out_weight.shape, bf16),
            pltpu.VMEM((batch_size, devices, positions, 2 * kv_local * HD), bf16),
            pltpu.VMEM((kv_local, rows, HD), bf16),
            pltpu.VMEM((kv_local, rows, HD), f32),
            pltpu.VMEM((kv_local, rows, HD), f32),
            pltpu.VMEM((kv_local, rows, HD), f32),
            pltpu.VMEM((batch_size, positions, heads_local * HD), bf16),
            pair, pair, far, far,
            pltpu.VMEM((steps, STEP_ROWS, width), f32),
            pltpu.VMEM((batch_size, positions, width), bf16),
            dma((3,)),
            dma((reached,)),
            dma((reached, max(columns - 1, 1))),
            dma((batch_size,)),
            dma((reached, columns, PIECES)),
            dma((steps,)), dma((2 * (positions // STEP_ROWS),)),
            dma((chips - 1, steps)), dma((chips - 1, steps)),
        ],
        compiler_params=pltpu.CompilerParams(
            collective_id=collective_id, has_side_effects=True, vmem_limit_bytes=56 * 2**20
        ),
    )(slot, x, key_value_weight, query_weight, out_weight, chosen)


def prepare_kernel(
    short, whole, columns, length_hbm, x_hbm, wk_hbm, wv_hbm,
    slot_ref, x_ref, wkv_ref, length_ref, load_sem,
):
    batch_size, positions, _ = x_ref.shape
    half = wkv_ref.shape[1] // 2
    first = lax.axis_index("kv") // columns * columns
    loads = [
        pltpu.make_async_copy(length_hbm, length_ref, load_sem.at[0]),
        pltpu.make_async_copy(wk_hbm, wkv_ref.at[:, pl.ds(0, half)], load_sem.at[1]),
        pltpu.make_async_copy(wv_hbm, wkv_ref.at[:, pl.ds(half, half)], load_sem.at[2]),
    ]
    for load in loads:
        load.start()
    loads[0].wait()

    lengths = [length_ref[b] for b in range(batch_size)]
    ranks = []
    for b in range(batch_size):
        ahead = [
            (lengths[o] >= lengths[b] if o < b else lengths[o] > lengths[b]).astype(jnp.int32)
            for o in range(batch_size) if o != b
        ]
        ranks.append(sum(ahead))
    slots = range(batch_size)
    held = [sum([jnp.where(ranks[b] == j, b, 0) for b in slots]) for j in slots]
    spans = [sum([jnp.where(ranks[b] == j, lengths[b], 0) for b in slots]) for j in slots]
    fits = jnp.int32(1)
    for j in slots:
        fits = fits * (spans[j] <= short[j] * positions).astype(jnp.int32)

    def x_load(j):
        return pltpu.make_async_copy(x_hbm.at[held[j]], x_ref.at[j], load_sem.at[3 + j])

    used = [first < jnp.where(fits > 0, short[j], whole[j]) for j in slots]
    for j in slots:
        @pl.when(used[j])
        def _():
            x_load(j).start()

    slot_ref[0] = fits
    for j in slots:
        slot_ref[1 + j] = held[j]
        slot_ref[1 + batch_size + j] = ranks[j]
        slot_ref[1 + 2 * batch_size + j] = spans[j]
    loads[1].wait()
    loads[2].wait()
    for j in slots:
        @pl.when(used[j])
        def _():
            x_load(j).wait()


def shards(inputs, query_weight, key_weight, value_weight, out_weight, chosen, lengths):
    batch_size, positions, model_width = inputs.shape
    devices = lax.axis_size("kv")
    short, whole = spans(batch_size, devices, positions)
    hbm = pl.BlockSpec(memory_space=pl.ANY)
    vmem = pl.BlockSpec(memory_space=pltpu.VMEM)
    smem = pl.BlockSpec(memory_space=pltpu.SMEM)
    slot, x, key_value_weight = pl.pallas_call(
        functools.partial(prepare_kernel, short, whole, columns_of(devices)),
        out_shape=(
            pltpu.SMEM((1 + 3 * batch_size,), jnp.int32),
            pltpu.VMEM(inputs.shape, inputs.dtype),
            pltpu.VMEM((model_width, 2 * key_weight.shape[1]), key_weight.dtype),
        ),
        in_specs=[hbm] * 4,
        out_specs=(smem, vmem, vmem),
        scratch_shapes=[
            pltpu.SMEM(lengths.shape, jnp.int32),
            pltpu.SemaphoreType.DMA((3 + batch_size,)),
        ],
        compiler_params=pltpu.CompilerParams(vmem_limit_bytes=57 * 2**20),
    )(lengths, inputs, key_weight, value_weight)
    return lax.cond(
        slot[0] > 0,
        functools.partial(layer, short, 0),
        functools.partial(layer, whole, 1),
        slot, x, key_value_weight, query_weight, out_weight, chosen,
    )


def solution(mesh):
    placed = (
        P(None, "kv", None),
        P(None, "tp"),
        P(None, "tp"),
        P(None, "tp"),
        P("tp", None),
        P(None, "kv", None),
        P(),
    )
    return jax.shard_map(
        shards, mesh=mesh, in_specs=placed, out_specs=P(None, "kv", "tp"), check_vma=False
    )
```

```python
import functools

import jax
import jax.numpy as jnp
from jax import lax
from jax.experimental import pallas as pl
from jax.experimental.pallas import tpu as pltpu
from jax.sharding import PartitionSpec as P

HD = 128
KB = 64
MASKED = -1e30
PIECES = 4
STEP_ROWS = 128
MESH = pl.DeviceIdType.MESH


def spans(batch_size, devices, positions):
    seq = devices * positions
    total = seq + seq // 2
    longest = [min(seq, (total - (batch_size - 1 - j)) // (j + 1)) for j in range(batch_size)]
    whole = tuple(-(-length // positions) for length in longest)
    short = tuple(
        min(full, -(-devices * 3 // (8 * j)) if j else devices) for j, full in enumerate(whole)
    )
    return short, whole


def layer_kernel(
    reach, columns, kv_local, per_group, tp,
    slot_ref, x_ref, wkv_ref, wq_hbm, wo_hbm, chosen_hbm, out_ref,
    chosen_ref, wq_ref, wo_ref, kv_ref, q_ref,
    top_ref, total_ref, acc_ref, att_ref,
    pair_out, pair_in, far_out, far_in, near, mixed_ref,
    load_sem, z_sent, x_sent, aside, z_got, x_got, pair_sent, pair_got, far_sent, far_got,
):
    batch_size, positions, _ = x_ref.shape
    slots, devices = kv_ref.shape[:2]
    rows_z = devices // columns
    per_dev = positions // KB
    half = kv_local * HD
    rows = per_group * positions
    width = out_ref.shape[-1]
    piece_rows = positions // PIECES
    mix_steps = positions // STEP_ROWS
    scaling = HD ** (-0.5)
    contract = (((1,), (1,)), ((), ()))

    device = lax.axis_index("kv")
    z = device // columns
    x = lax.rem(device, columns)
    me = lax.axis_index("tp")
    core = lax.rem(me, 2)
    chip = me // 2
    chips = tp // 2
    partner = me + 1 - 2 * core

    def live_at(r):
        return sum([(r < reach[j]).astype(jnp.int32) for j in range(slots)])

    def column(i):
        return lax.rem(x + i, columns)

    def twin(off):
        return lax.rem(chip + off, chips) * 2 + core

    mine = live_at(device)
    row_live = live_at(z * columns)
    next_live = live_at((z + 1) * columns)

    loads = [
        pltpu.make_async_copy(wq_hbm, wq_ref, load_sem.at[0]),
        pltpu.make_async_copy(chosen_hbm, chosen_ref, load_sem.at[1]),
        pltpu.make_async_copy(wo_hbm, wo_ref, load_sem.at[2]),
    ]
    for load in loads:
        load.start()

    barrier = pltpu.get_barrier_semaphore()

    def greet(**where):
        pl.semaphore_signal(barrier, inc=1, device_id=where, device_id_type=MESH)

    greet(tp=partner)
    for off in range(1, chips):
        greet(tp=twin(off))
    for i in range(1, columns):
        greet(kv=z * columns + column(i))

    @pl.when(z > 0)
    def _():
        greet(kv=device - columns)

    @pl.when(z < rows_z - 1)
    def _():
        greet(kv=device + columns)

    def holder(j):
        return slot_ref[1 + j]

    def at_slot(j, row):
        return row + sum(
            [jnp.where(k < j, -(-reach[k] // columns), 0) for k in range(slots - 1)]
        )

    def part(j, c, p, n):
        return kv_ref.at[j, c, pl.ds(p * piece_rows, n * piece_rows)]

    def send(j, c, p, n, sent, landed, where):
        return pltpu.make_async_remote_copy(
            src_ref=part(j, c, p, n), dst_ref=part(j, c, p, n), send_sem=sent,
            recv_sem=landed, device_id=where, device_id_type=MESH,
        )

    def z_copy(j, c, p, n=1):
        at = at_slot(j, c // columns)
        return send(j, c, p, n, z_sent.at[at], z_got.at[at, p], {"kv": device + columns})

    def x_copy(j, c, p, i, n=1):
        at = at_slot(j, c // columns)
        return send(
            j, c, p, n, x_sent.at[at, i - 1], x_got.at[at, columns - i - 1],
            {"kv": z * columns + column(i)},
        )

    def aside_copy(j):
        first = PIECES // 2
        return send(
            j, device - 1, first, PIECES - first, aside.at[j],
            x_got.at[at_slot(j, z), columns - 2], {"kv": device + columns},
        )

    def z_arrival(j, c, p):
        at = at_slot(j, c // columns)
        return send(j, c, p, 1, z_sent.at[at], z_got.at[at, p], {"tp": partner})

    def x_arrival(j, c, i):
        at = at_slot(j, c // columns)
        return send(j, c, 0, PIECES, z_sent.at[at], x_got.at[at, i - 1], {"tp": partner})

    def by_z(c, i):
        return (c == device - columns) & (x == 0) & (column(i) == 1)

    def to_row(j, c, i):
        own = c == device
        return (j < live_at(z * columns + column(i))) & (
            jnp.logical_not(own) | (column(i) > x)
        )

    def each_send(j, c, p):
        @pl.when(j < next_live)
        def _():
            z_copy(j, c, p).start()

        for i in range(1, columns):
            wanted = to_row(j, c, i)
            if p >= PIECES // 2:
                wanted = wanted & jnp.logical_not(by_z(c, i))

            @pl.when(wanted)
            def _():
                x_copy(j, c, p, i).start()

    def each_sent(j, c):
        @pl.when(j < next_live)
        def _():
            z_copy(j, c, 0, PIECES).wait_send()

        for i in range(1, columns):
            @pl.when(to_row(j, c, i) & by_z(c, i))
            def _():
                x_copy(j, c, 0, i, PIECES // 2).wait_send()

            @pl.when(to_row(j, c, i) & jnp.logical_not(by_z(c, i)))
            def _():
                x_copy(j, c, 0, i, PIECES).wait_send()

    def put_aside(j, act):
        @pl.when((x == 1) & (j < live_at(device + columns)))
        def _():
            act(aside_copy(j))

    def send_own(j):
        for p in range(PIECES):
            each_send(j, device, p)

    def project_kv(j, carry):
        kv_ref[j, device] = jnp.dot(
            x_ref[j], wkv_ref[...], preferred_element_type=jnp.float32
        ).astype(jnp.bfloat16)

        @pl.when(j == 0)
        def _():
            pl.semaphore_wait(
                barrier,
                chips + columns - 1
                + (z > 0).astype(jnp.int32) + (z < rows_z - 1).astype(jnp.int32),
            )

        @pl.when((j == 0) | (z == 0))
        def _():
            send_own(j)

        return carry

    lax.fori_loop(0, jnp.where(z == 0, 1, row_live), project_kv, 0)
    loads[0].wait()
    loads[1].wait()

    def project_q(j):
        queries = jnp.dot(
            x_ref[j], wq_ref[...], preferred_element_type=jnp.float32
        ).astype(jnp.bfloat16)
        for n in range(kv_local * per_group):
            h, g = n // per_group, n % per_group
            q_ref[h, g * positions:(g + 1) * positions, :] = queries[:, n * HD:(n + 1) * HD]

    def named(names, c):
        segment = lax.broadcasted_iota(jnp.int32, (per_dev, positions), 1) // KB
        bias = jnp.full((per_dev, positions), MASKED, jnp.float32)
        for i in range(per_dev):
            hit = jnp.max(
                jnp.where(names == c * per_dev + i, 0.0, MASKED), axis=1, keepdims=True
            )
            bias = jnp.where(segment == i, hit, bias)
        return jnp.broadcast_to(bias[:, None, :], (per_dev, KB, positions)).reshape(
            positions, positions
        )

    def scores(j, c, h, bias):
        raw = lax.dot_general(
            q_ref[h], kv_ref[j, c, :, h * HD:(h + 1) * HD], contract,
            preferred_element_type=jnp.float32,
        )
        shaped = (raw * scaling).reshape(per_group, positions, positions) + bias[None]
        return shaped.reshape(rows, positions)

    def weigh(j, c, h, raised):
        return jnp.dot(
            raised.astype(jnp.bfloat16), kv_ref[j, c, :, half + h * HD:half + (h + 1) * HD],
            preferred_element_type=jnp.float32,
        )

    def wide(value):
        return jnp.concatenate([value] * (positions // HD), axis=1)

    def attend_own(j):
        names = chosen_ref[holder(j)]
        before = named(names, device)
        home = device * per_dev + lax.broadcasted_iota(jnp.int32, names.shape, 0)
        copies = jnp.sum(jnp.where(names == home, 1.0, 0.0), axis=1, keepdims=True)
        same = jnp.log(jnp.maximum(copies, 1.0))
        same = jnp.broadcast_to(same[:, None, :], (per_dev, KB, positions)).reshape(
            positions, positions
        )
        at_row = lax.broadcasted_iota(jnp.int32, (positions, positions), 0)
        at_col = lax.broadcasted_iota(jnp.int32, (positions, positions), 1)
        bias = jnp.where(at_col < at_row, before, jnp.where(at_col == at_row, same, MASKED))
        for h in range(kv_local):
            s = scores(j, device, h, bias)
            top = jnp.broadcast_to(jnp.max(s, axis=1, keepdims=True), (rows, HD))
            raised = jnp.exp(s - wide(top))
            top_ref[h] = top
            total_ref[h] = jnp.broadcast_to(jnp.sum(raised, axis=1, keepdims=True), (rows, HD))
            acc_ref[h] = weigh(j, device, h, raised)

    def attend_far(j, c):
        bias = named(chosen_ref[holder(j)], c)
        for h in range(kv_local):
            s = scores(j, c, h, bias)
            old = top_ref[h]
            top = jnp.maximum(old, jnp.max(s, axis=1, keepdims=True))
            fade = jnp.exp(old - top)
            raised = jnp.exp(s - wide(top))
            top_ref[h] = top
            total_ref[h] = total_ref[h] * fade + jnp.sum(raised, axis=1, keepdims=True)
            acc_ref[h] = acc_ref[h] * fade + weigh(j, c, h, raised)

    def attend_end(j):
        live = slot_ref[1 + 2 * batch_size + j] - device * positions
        living = lax.broadcasted_iota(jnp.int32, (positions, HD), 0) < live
        for h in range(kv_local):
            done = acc_ref[h] / total_ref[h]
            for g in range(per_group):
                n = h * per_group + g
                att_ref[j, :, n * HD:(n + 1) * HD] = jnp.where(
                    living, done[g * positions:(g + 1) * positions], 0.0
                ).astype(jnp.bfloat16)

    def group_sum(j, m, off, side):
        start = (lax.rem(chip + off, chips) * 2 + side) * width
        return jnp.dot(
            att_ref[j, m * STEP_ROWS:(m + 1) * STEP_ROWS, :],
            wo_ref[:, pl.ds(pl.multiple_of(start, width), width)],
            preferred_element_type=jnp.float32,
        ).astype(jnp.bfloat16)

    def pair_copy(i):
        return pltpu.make_async_remote_copy(
            src_ref=pair_out.at[i], dst_ref=pair_in.at[i],
            send_sem=pair_sent.at[i], recv_sem=pair_got.at[lax.rem(i, 2 * mix_steps)],
            device_id={"tp": partner}, device_id_type=MESH,
        )

    def far_copy(i, off):
        return pltpu.make_async_remote_copy(
            src_ref=far_out.at[off - 1, i], dst_ref=far_in.at[off - 1, i],
            send_sem=far_sent.at[off - 1, i], recv_sem=far_got.at[off - 1, i],
            device_id={"tp": twin(off)}, device_id_type=MESH,
        )

    def mix(j):
        for m in range(mix_steps):
            i = j * mix_steps + m
            for off in range(chips):
                pair_out[i, off] = group_sum(j, m, off, 1 - core)
            pair_copy(i).start()
        for m in range(mix_steps):
            i = j * mix_steps + m
            sums = [group_sum(j, m, off, core).astype(jnp.float32) for off in range(chips)]
            pair_copy(i).wait_recv()
            for off in range(1, chips):
                both = sums[off] + pair_in[i, off].astype(jnp.float32)
                far_out[off - 1, i] = both.astype(jnp.bfloat16)
                far_copy(i, off).start()
            near[i] = sums[0] + pair_in[i, 0].astype(jnp.float32)

    def relay(t, between=None):
        j = t // z
        d = lax.rem(t, z)
        c = device - (d + 1) * columns

        @pl.when((d == 0) & (j > 0))
        def _():
            send_own(j)

        for p in range(PIECES):
            z_arrival(j, c, p).wait_recv()
            each_send(j, c, p)
            if p == 0 and between is not None:
                between()

    def take(j, c, i):
        x_arrival(j, c, i).wait_recv()
        attend_far(j, c)

    def slot(j, carry):
        used = j < mine

        @pl.when(used)
        def _():
            project_q(j)
            attend_own(j)

        @pl.when((z == 0) & (j + 1 < row_live))
        def _():
            project_kv(j + 1, 0)

        @pl.when(j == 0)
        def _():
            loads[2].wait()

        @pl.when((j == 0) & (z > 0))
        def _():
            relay(0)

        def step(t, carry):
            d = t // columns
            i = lax.rem(t, columns)
            ahead = j * z + d
            below = (i == 0) & (d > 0) & (d <= z)

            @pl.when((z > 0) & (i == 0) & (d == jnp.maximum(z, 2)))
            def _():
                put_aside(j, lambda copy: copy.start())

            def attend_below():
                @pl.when(used)
                def _():
                    attend_far(j, device - d * columns)

            @pl.when(below & (ahead < row_live * z))
            def _():
                relay(ahead, attend_below)

            @pl.when(below & (ahead >= row_live * z))
            def _():
                attend_below()

            other = column(i)
            late = (x == 1) & (other == 0)
            last = d - 1
            turn = jnp.where(last == z, z, jnp.where(last == z - 1, 1, last + 1))
            back = jnp.where(late & (last > 0), turn, last)

            @pl.when(used & (i > 0) & (d > 0) & ((last > 0) | (other < x)))
            def _():
                take(j, (z - back) * columns + other, jnp.maximum(i, 1))

            return carry

        lax.fori_loop(0, (z + 2) * columns, step, 0)

        @pl.when(z == 0)
        def _():
            put_aside(j, lambda copy: copy.start())

        @pl.when(used)
        def _():
            attend_end(j)
            mix(j)

        return carry

    lax.fori_loop(0, row_live, slot, 0)

    def finish(j, carry):
        for m in range(mix_steps):
            i = j * mix_steps + m
            pair_copy(i).wait_send()
            mixed = near[i]
            for off in range(1, chips):
                far_copy(i, off).wait()
                mixed = mixed + far_in[off - 1, i].astype(jnp.float32)
            mixed_ref[j, m * STEP_ROWS:(m + 1) * STEP_ROWS, :] = mixed.astype(jnp.bfloat16)
        return carry

    lax.fori_loop(0, mine, finish, 0)

    def blank(j, carry):
        mixed_ref[j] = jnp.zeros(mixed_ref.shape[1:], jnp.bfloat16)
        return carry

    lax.fori_loop(mine, slots, blank, 0)
    for b in range(batch_size):
        out_ref[b] = mixed_ref[slot_ref[1 + batch_size + b]]

    def drain(j, carry):
        def back(d, carry):
            c = (z - d) * columns + x
            each_sent(j, c)
            return carry

        put_aside(j, lambda copy: copy.wait_send())
        return lax.fori_loop(0, z + 1, back, carry)

    lax.fori_loop(0, row_live, drain, 0)


def columns_of(devices):
    return 1 << ((devices.bit_length() - 1) // 2)


def layer(
    reach, collective_id, slot, x, key_value_weight,
    query_weight, out_weight, chosen,
):
    batch_size, positions, _ = x.shape
    kv_local = key_value_weight.shape[1] // (2 * HD)
    heads_local = query_weight.shape[1] // HD
    per_group = heads_local // kv_local
    devices = lax.axis_size("kv")
    tp = lax.axis_size("tp")
    chips = tp // 2
    columns = columns_of(devices)
    width = out_weight.shape[1] // tp
    steps = batch_size * (positions // STEP_ROWS)
    rows = per_group * positions
    reached = sum([-(-span // columns) for span in reach])
    bf16, f32 = jnp.bfloat16, jnp.float32
    vmem = pl.BlockSpec(memory_space=pltpu.VMEM)
    smem = pl.BlockSpec(memory_space=pltpu.SMEM)
    hbm = pl.BlockSpec(memory_space=pl.ANY)
    dma = pltpu.SemaphoreType.DMA
    pair = pltpu.VMEM((steps, chips, STEP_ROWS, width), bf16)
    far = pltpu.VMEM((chips - 1, steps, STEP_ROWS, width), bf16)
    return pl.pallas_call(
        functools.partial(layer_kernel, reach, columns, kv_local, per_group, tp),
        out_shape=jax.ShapeDtypeStruct((batch_size, positions, width), bf16),
        in_specs=[smem, vmem, vmem, hbm, hbm, hbm],
        out_specs=vmem,
        scratch_shapes=[
            pltpu.VMEM(chosen.shape, jnp.int32),
            pltpu.VMEM(query_weight.shape, bf16),
            pltpu.VMEM(out_weight.shape, bf16),
            pltpu.VMEM((batch_size, devices, positions, 2 * kv_local * HD), bf16),
            pltpu.VMEM((kv_local, rows, HD), bf16),
            pltpu.VMEM((kv_local, rows, HD), f32),
            pltpu.VMEM((kv_local, rows, HD), f32),
            pltpu.VMEM((kv_local, rows, HD), f32),
            pltpu.VMEM((batch_size, positions, heads_local * HD), bf16),
            pair, pair, far, far,
            pltpu.VMEM((steps, STEP_ROWS, width), f32),
            pltpu.VMEM((batch_size, positions, width), bf16),
            dma((3,)),
            dma((reached,)),
            dma((reached, max(columns - 1, 1))),
            dma((batch_size,)),
            dma((reached, PIECES)),
            dma((reached, max(columns - 1, 1))),
            dma((steps,)), dma((2 * (positions // STEP_ROWS),)),
            dma((chips - 1, steps)), dma((chips - 1, steps)),
        ],
        compiler_params=pltpu.CompilerParams(
            collective_id=collective_id, has_side_effects=True, vmem_limit_bytes=56 * 2**20
        ),
    )(slot, x, key_value_weight, query_weight, out_weight, chosen)


def prepare_kernel(
    short, whole, columns, length_hbm, x_hbm, wk_hbm, wv_hbm,
    slot_ref, x_ref, wkv_ref, length_ref, load_sem,
):
    batch_size, positions, _ = x_ref.shape
    half = wkv_ref.shape[1] // 2
    first = lax.axis_index("kv") // columns * columns
    loads = [
        pltpu.make_async_copy(length_hbm, length_ref, load_sem.at[0]),
        pltpu.make_async_copy(wk_hbm, wkv_ref.at[:, pl.ds(0, half)], load_sem.at[1]),
        pltpu.make_async_copy(wv_hbm, wkv_ref.at[:, pl.ds(half, half)], load_sem.at[2]),
    ]
    for load in loads:
        load.start()
    loads[0].wait()

    lengths = [length_ref[b] for b in range(batch_size)]
    ranks = []
    for b in range(batch_size):
        ahead = [
            (lengths[o] >= lengths[b] if o < b else lengths[o] > lengths[b]).astype(jnp.int32)
            for o in range(batch_size) if o != b
        ]
        ranks.append(sum(ahead))
    slots = range(batch_size)
    held = [sum([jnp.where(ranks[b] == j, b, 0) for b in slots]) for j in slots]
    spans = [sum([jnp.where(ranks[b] == j, lengths[b], 0) for b in slots]) for j in slots]
    fits = jnp.int32(1)
    for j in slots:
        fits = fits * (spans[j] <= short[j] * positions).astype(jnp.int32)

    def x_load(j):
        return pltpu.make_async_copy(x_hbm.at[held[j]], x_ref.at[j], load_sem.at[3 + j])

    used = [first < jnp.where(fits > 0, short[j], whole[j]) for j in slots]
    for j in slots:
        @pl.when(used[j])
        def _():
            x_load(j).start()

    slot_ref[0] = fits
    for j in slots:
        slot_ref[1 + j] = held[j]
        slot_ref[1 + batch_size + j] = ranks[j]
        slot_ref[1 + 2 * batch_size + j] = spans[j]
    loads[1].wait()
    loads[2].wait()
    for j in slots:
        @pl.when(used[j])
        def _():
            x_load(j).wait()


def shards(inputs, query_weight, key_weight, value_weight, out_weight, chosen, lengths):
    batch_size, positions, model_width = inputs.shape
    devices = lax.axis_size("kv")
    short, whole = spans(batch_size, devices, positions)
    hbm = pl.BlockSpec(memory_space=pl.ANY)
    vmem = pl.BlockSpec(memory_space=pltpu.VMEM)
    smem = pl.BlockSpec(memory_space=pltpu.SMEM)
    slot, x, key_value_weight = pl.pallas_call(
        functools.partial(prepare_kernel, short, whole, columns_of(devices)),
        out_shape=(
            pltpu.SMEM((1 + 3 * batch_size,), jnp.int32),
            pltpu.VMEM(inputs.shape, inputs.dtype),
            pltpu.VMEM((model_width, 2 * key_weight.shape[1]), key_weight.dtype),
        ),
        in_specs=[hbm] * 4,
        out_specs=(smem, vmem, vmem),
        scratch_shapes=[
            pltpu.SMEM(lengths.shape, jnp.int32),
            pltpu.SemaphoreType.DMA((3 + batch_size,)),
        ],
        compiler_params=pltpu.CompilerParams(vmem_limit_bytes=57 * 2**20),
    )(lengths, inputs, key_weight, value_weight)
    return lax.cond(
        slot[0] > 0,
        functools.partial(layer, short, 0),
        functools.partial(layer, whole, 1),
        slot, x, key_value_weight, query_weight, out_weight, chosen,
    )


def solution(mesh):
    placed = (
        P(None, "kv", None),
        P(None, "tp"),
        P(None, "tp"),
        P(None, "tp"),
        P("tp", None),
        P(None, "kv", None),
        P(),
    )
    return jax.shard_map(
        shards, mesh=mesh, in_specs=placed, out_specs=P(None, "kv", "tp"), check_vma=False
    )
```

```python
import functools

import jax
import jax.numpy as jnp
from jax import lax
from jax.experimental import pallas as pl
from jax.experimental.pallas import tpu as pltpu
from jax.sharding import PartitionSpec as P

HD = 128
KB = 64
MASKED = -1e30
PIECES = 4
STEP_ROWS = 128
MESH = pl.DeviceIdType.MESH


def spans(batch_size, devices, positions):
    seq = devices * positions
    total = seq + seq // 2
    longest = [min(seq, (total - (batch_size - 1 - j)) // (j + 1)) for j in range(batch_size)]
    whole = tuple(-(-length // positions) for length in longest)
    short = tuple(
        min(full, -(-devices * 3 // (8 * j)) if j else devices) for j, full in enumerate(whole)
    )
    return short, whole


def layer_kernel(
    reach, columns, kv_local, per_group, tp,
    slot_ref, x_ref, wkv_ref, wq_hbm, wo_hbm, chosen_hbm, out_ref,
    chosen_ref, wq_ref, wo_ref, kv_ref, q_ref,
    top_ref, total_ref, acc_ref, att_ref,
    pair_out, pair_in, far_out, far_in, near, mixed_ref,
    load_sem, z_sent, x_sent, aside, z_got, x_got, pair_sent, pair_got, far_sent, far_got,
):
    batch_size, positions, _ = x_ref.shape
    slots, devices = kv_ref.shape[:2]
    rows_z = devices // columns
    per_dev = positions // KB
    half = kv_local * HD
    rows = per_group * positions
    width = out_ref.shape[-1]
    piece_rows = positions // PIECES
    mix_steps = positions // STEP_ROWS
    scaling = HD ** (-0.5)
    contract = (((1,), (1,)), ((), ()))

    device = lax.axis_index("kv")
    z = device // columns
    x = lax.rem(device, columns)
    me = lax.axis_index("tp")
    core = lax.rem(me, 2)
    chip = me // 2
    chips = tp // 2
    partner = me + 1 - 2 * core

    def live_at(r):
        return sum([(r < reach[j]).astype(jnp.int32) for j in range(slots)])

    def column(i):
        return lax.rem(x + i, columns)

    def twin(off):
        return lax.rem(chip + off, chips) * 2 + core

    mine = live_at(device)
    row_live = live_at(z * columns)
    next_live = live_at((z + 1) * columns)

    loads = [
        pltpu.make_async_copy(wq_hbm, wq_ref, load_sem.at[0]),
        pltpu.make_async_copy(chosen_hbm, chosen_ref, load_sem.at[1]),
        pltpu.make_async_copy(wo_hbm, wo_ref, load_sem.at[2]),
    ]
    for load in loads:
        load.start()

    barrier = pltpu.get_barrier_semaphore()

    def greet(**where):
        pl.semaphore_signal(barrier, inc=1, device_id=where, device_id_type=MESH)

    greet(tp=partner)
    for off in range(1, chips):
        greet(tp=twin(off))
    for i in range(1, columns):
        greet(kv=z * columns + column(i))

    @pl.when(z > 0)
    def _():
        greet(kv=device - columns)

    @pl.when(z < rows_z - 1)
    def _():
        greet(kv=device + columns)

    def holder(j):
        return slot_ref[1 + j]

    def at_slot(j, row):
        return row + sum(
            [jnp.where(k < j, -(-reach[k] // columns), 0) for k in range(slots - 1)]
        )

    def part(j, c, p, n):
        return kv_ref.at[j, c, pl.ds(p * piece_rows, n * piece_rows)]

    def send(j, c, p, n, sent, landed, where):
        return pltpu.make_async_remote_copy(
            src_ref=part(j, c, p, n), dst_ref=part(j, c, p, n), send_sem=sent,
            recv_sem=landed, device_id=where, device_id_type=MESH,
        )

    def z_copy(j, c, p, n=1):
        at = at_slot(j, c // columns)
        return send(j, c, p, n, z_sent.at[at], z_got.at[at, p], {"kv": device + columns})

    def x_copy(j, c, p, i, n=1):
        at = at_slot(j, c // columns)
        return send(
            j, c, p, n, x_sent.at[at, i - 1], x_got.at[at, columns - i - 1],
            {"kv": z * columns + column(i)},
        )

    def aside_copy(j):
        first = PIECES // 2
        return send(
            j, device - 1, first, PIECES - first, aside.at[j],
            x_got.at[at_slot(j, z), columns - 2], {"kv": device + columns},
        )

    def z_arrival(j, c, p):
        at = at_slot(j, c // columns)
        return send(j, c, p, 1, z_sent.at[at], z_got.at[at, p], {"tp": partner})

    def x_arrival(j, c, i):
        at = at_slot(j, c // columns)
        return send(j, c, 0, PIECES, z_sent.at[at], x_got.at[at, i - 1], {"tp": partner})

    def by_z(c, i):
        return (c == device - columns) & (x == 0) & (column(i) == 1)

    def to_row(j, c, i):
        own = c == device
        return (j < live_at(z * columns + column(i))) & (
            jnp.logical_not(own) | (column(i) > x)
        )

    def each_send(j, c, p):
        @pl.when(j < next_live)
        def _():
            z_copy(j, c, p).start()

        for i in range(1, columns):
            wanted = to_row(j, c, i)
            if p >= PIECES // 2:
                wanted = wanted & jnp.logical_not(by_z(c, i))

            @pl.when(wanted)
            def _():
                x_copy(j, c, p, i).start()

    def each_sent(j, c):
        @pl.when(j < next_live)
        def _():
            z_copy(j, c, 0, PIECES).wait_send()

        for i in range(1, columns):
            @pl.when(to_row(j, c, i) & by_z(c, i))
            def _():
                x_copy(j, c, 0, i, PIECES // 2).wait_send()

            @pl.when(to_row(j, c, i) & jnp.logical_not(by_z(c, i)))
            def _():
                x_copy(j, c, 0, i, PIECES).wait_send()

    def put_aside(j, act):
        @pl.when((x == 1) & (j < live_at(device + columns)))
        def _():
            act(aside_copy(j))

    def send_own(j):
        for p in range(PIECES):
            each_send(j, device, p)

    def project_kv(j, carry):
        kv_ref[j, device] = jnp.dot(
            x_ref[j], wkv_ref[...], preferred_element_type=jnp.float32
        ).astype(jnp.bfloat16)

        @pl.when(j == 0)
        def _():
            pl.semaphore_wait(
                barrier,
                chips + columns - 1
                + (z > 0).astype(jnp.int32) + (z < rows_z - 1).astype(jnp.int32),
            )

        @pl.when((j == 0) | (z == 0))
        def _():
            send_own(j)

        return carry

    lax.fori_loop(0, jnp.where(z == 0, 1, row_live), project_kv, 0)
    loads[0].wait()
    loads[1].wait()

    def project_q(j):
        queries = jnp.dot(
            x_ref[j], wq_ref[...], preferred_element_type=jnp.float32
        ).astype(jnp.bfloat16)
        for n in range(kv_local * per_group):
            h, g = n // per_group, n % per_group
            q_ref[h, g * positions:(g + 1) * positions, :] = queries[:, n * HD:(n + 1) * HD]

    def named(names, c):
        segment = lax.broadcasted_iota(jnp.int32, (per_dev, positions), 1) // KB
        bias = jnp.full((per_dev, positions), MASKED, jnp.float32)
        for i in range(per_dev):
            hit = jnp.max(
                jnp.where(names == c * per_dev + i, 0.0, MASKED), axis=1, keepdims=True
            )
            bias = jnp.where(segment == i, hit, bias)
        return bias

    def by_row(bias):
        return jnp.broadcast_to(bias[:, None, :], (per_dev, KB, positions)).reshape(
            positions, positions
        )

    def scores(j, c, h, bias):
        raw = lax.dot_general(
            q_ref[h], kv_ref[j, c, :, h * HD:(h + 1) * HD], contract,
            preferred_element_type=jnp.float32,
        )
        shaped = (raw * scaling).reshape(per_group, positions, positions) + bias[None]
        return shaped.reshape(rows, positions)

    def weigh(j, c, h, raised):
        return jnp.dot(
            raised.astype(jnp.bfloat16), kv_ref[j, c, :, half + h * HD:half + (h + 1) * HD],
            preferred_element_type=jnp.float32,
        )

    def wide(value):
        return jnp.concatenate([value] * (positions // HD), axis=1)

    def attend_own(j):
        names = chosen_ref[holder(j)]
        before = by_row(named(names, device))
        home = device * per_dev + lax.broadcasted_iota(jnp.int32, names.shape, 0)
        copies = jnp.sum(jnp.where(names == home, 1.0, 0.0), axis=1, keepdims=True)
        same = jnp.log(jnp.maximum(copies, 1.0))
        same = jnp.broadcast_to(same[:, None, :], (per_dev, KB, positions)).reshape(
            positions, positions
        )
        at_row = lax.broadcasted_iota(jnp.int32, (positions, positions), 0)
        at_col = lax.broadcasted_iota(jnp.int32, (positions, positions), 1)
        bias = jnp.where(at_col < at_row, before, jnp.where(at_col == at_row, same, MASKED))
        for h in range(kv_local):
            s = scores(j, device, h, bias)
            top = jnp.broadcast_to(jnp.max(s, axis=1, keepdims=True), (rows, HD))
            raised = jnp.exp(s - wide(top))
            top_ref[h] = top
            total_ref[h] = jnp.broadcast_to(jnp.sum(raised, axis=1, keepdims=True), (rows, HD))
            acc_ref[h] = weigh(j, device, h, raised)

    def attend_far(j, c, arrive=None):
        bias = named(chosen_ref[holder(j)], c)
        if arrive is not None:
            arrive()
        bias = by_row(bias)
        for h in range(kv_local):
            s = scores(j, c, h, bias)
            old = top_ref[h]
            top = jnp.maximum(old, jnp.max(s, axis=1, keepdims=True))
            fade = jnp.exp(old - top)
            raised = jnp.exp(s - wide(top))
            top_ref[h] = top
            total_ref[h] = total_ref[h] * fade + jnp.sum(raised, axis=1, keepdims=True)
            acc_ref[h] = acc_ref[h] * fade + weigh(j, c, h, raised)

    def attend_end(j):
        live = slot_ref[1 + 2 * batch_size + j] - device * positions
        living = lax.broadcasted_iota(jnp.int32, (positions, HD), 0) < live
        for h in range(kv_local):
            done = acc_ref[h] / total_ref[h]
            for g in range(per_group):
                n = h * per_group + g
                att_ref[j, :, n * HD:(n + 1) * HD] = jnp.where(
                    living, done[g * positions:(g + 1) * positions], 0.0
                ).astype(jnp.bfloat16)

    def group_sum(j, m, off, side):
        start = (lax.rem(chip + off, chips) * 2 + side) * width
        return jnp.dot(
            att_ref[j, m * STEP_ROWS:(m + 1) * STEP_ROWS, :],
            wo_ref[:, pl.ds(pl.multiple_of(start, width), width)],
            preferred_element_type=jnp.float32,
        ).astype(jnp.bfloat16)

    def pair_copy(i):
        return pltpu.make_async_remote_copy(
            src_ref=pair_out.at[i], dst_ref=pair_in.at[i],
            send_sem=pair_sent.at[i], recv_sem=pair_got.at[lax.rem(i, 2 * mix_steps)],
            device_id={"tp": partner}, device_id_type=MESH,
        )

    def far_copy(i, off):
        return pltpu.make_async_remote_copy(
            src_ref=far_out.at[off - 1, i], dst_ref=far_in.at[off - 1, i],
            send_sem=far_sent.at[off - 1, i], recv_sem=far_got.at[off - 1, i],
            device_id={"tp": twin(off)}, device_id_type=MESH,
        )

    def mix(j):
        for m in range(mix_steps):
            i = j * mix_steps + m
            for off in range(chips):
                pair_out[i, off] = group_sum(j, m, off, 1 - core)
            pair_copy(i).start()
        for m in range(mix_steps):
            i = j * mix_steps + m
            sums = [group_sum(j, m, off, core).astype(jnp.float32) for off in range(chips)]
            pair_copy(i).wait_recv()
            for off in range(1, chips):
                both = sums[off] + pair_in[i, off].astype(jnp.float32)
                far_out[off - 1, i] = both.astype(jnp.bfloat16)
                far_copy(i, off).start()
            near[i] = sums[0] + pair_in[i, 0].astype(jnp.float32)

    def relay(t, between=None):
        j = t // z
        d = lax.rem(t, z)
        c = device - (d + 1) * columns

        @pl.when((d == 0) & (j > 0))
        def _():
            send_own(j)

        for p in range(PIECES):
            z_arrival(j, c, p).wait_recv()
            each_send(j, c, p)
            if p == 0 and between is not None:
                between()

    def take(j, c, i):
        attend_far(j, c, lambda: x_arrival(j, c, i).wait_recv())

    def slot(j, carry):
        used = j < mine

        @pl.when(used)
        def _():
            project_q(j)
            attend_own(j)

        @pl.when((z == 0) & (j + 1 < row_live))
        def _():
            project_kv(j + 1, 0)

        @pl.when(j == 0)
        def _():
            loads[2].wait()

        @pl.when((j == 0) & (z > 0))
        def _():
            relay(0)

        def step(t, carry):
            d = t // columns
            i = lax.rem(t, columns)
            ahead = j * z + d
            below = (i == 0) & (d > 0) & (d <= z)

            @pl.when((z > 0) & (i == 0) & (d == jnp.maximum(z, 2)))
            def _():
                put_aside(j, lambda copy: copy.start())

            def attend_below():
                @pl.when(used)
                def _():
                    attend_far(j, device - d * columns)

            @pl.when(below & (ahead < row_live * z))
            def _():
                relay(ahead, attend_below)

            @pl.when(below & (ahead >= row_live * z))
            def _():
                attend_below()

            other = column(i)
            late = (x == 1) & (other == 0)
            last = d - 1
            turn = jnp.where(last == z, z, jnp.where(last == z - 1, 1, last + 1))
            back = jnp.where(late & (last > 0), turn, last)

            @pl.when(used & (i > 0) & (d > 0) & ((last > 0) | (other < x)))
            def _():
                take(j, (z - back) * columns + other, jnp.maximum(i, 1))

            return carry

        lax.fori_loop(0, (z + 2) * columns, step, 0)

        @pl.when(z == 0)
        def _():
            put_aside(j, lambda copy: copy.start())

        @pl.when(used)
        def _():
            attend_end(j)
            mix(j)

        return carry

    lax.fori_loop(0, row_live, slot, 0)

    def finish(j, carry):
        for m in range(mix_steps):
            i = j * mix_steps + m
            pair_copy(i).wait_send()
            mixed = near[i]
            for off in range(1, chips):
                far_copy(i, off).wait()
                mixed = mixed + far_in[off - 1, i].astype(jnp.float32)
            mixed_ref[j, m * STEP_ROWS:(m + 1) * STEP_ROWS, :] = mixed.astype(jnp.bfloat16)
        return carry

    lax.fori_loop(0, mine, finish, 0)

    def blank(j, carry):
        mixed_ref[j] = jnp.zeros(mixed_ref.shape[1:], jnp.bfloat16)
        return carry

    lax.fori_loop(mine, slots, blank, 0)
    for b in range(batch_size):
        out_ref[b] = mixed_ref[slot_ref[1 + batch_size + b]]

    def drain(j, carry):
        def back(d, carry):
            c = (z - d) * columns + x
            each_sent(j, c)
            return carry

        put_aside(j, lambda copy: copy.wait_send())
        return lax.fori_loop(0, z + 1, back, carry)

    lax.fori_loop(0, row_live, drain, 0)


def columns_of(devices):
    return 1 << ((devices.bit_length() - 1) // 2)


def layer(
    reach, collective_id, slot, x, key_value_weight,
    query_weight, out_weight, chosen,
):
    batch_size, positions, _ = x.shape
    kv_local = key_value_weight.shape[1] // (2 * HD)
    heads_local = query_weight.shape[1] // HD
    per_group = heads_local // kv_local
    devices = lax.axis_size("kv")
    tp = lax.axis_size("tp")
    chips = tp // 2
    columns = columns_of(devices)
    width = out_weight.shape[1] // tp
    steps = batch_size * (positions // STEP_ROWS)
    rows = per_group * positions
    reached = sum([-(-span // columns) for span in reach])
    bf16, f32 = jnp.bfloat16, jnp.float32
    vmem = pl.BlockSpec(memory_space=pltpu.VMEM)
    smem = pl.BlockSpec(memory_space=pltpu.SMEM)
    hbm = pl.BlockSpec(memory_space=pl.ANY)
    dma = pltpu.SemaphoreType.DMA
    pair = pltpu.VMEM((steps, chips, STEP_ROWS, width), bf16)
    far = pltpu.VMEM((chips - 1, steps, STEP_ROWS, width), bf16)
    return pl.pallas_call(
        functools.partial(layer_kernel, reach, columns, kv_local, per_group, tp),
        out_shape=jax.ShapeDtypeStruct((batch_size, positions, width), bf16),
        in_specs=[smem, vmem, vmem, hbm, hbm, hbm],
        out_specs=vmem,
        scratch_shapes=[
            pltpu.VMEM(chosen.shape, jnp.int32),
            pltpu.VMEM(query_weight.shape, bf16),
            pltpu.VMEM(out_weight.shape, bf16),
            pltpu.VMEM((batch_size, devices, positions, 2 * kv_local * HD), bf16),
            pltpu.VMEM((kv_local, rows, HD), bf16),
            pltpu.VMEM((kv_local, rows, HD), f32),
            pltpu.VMEM((kv_local, rows, HD), f32),
            pltpu.VMEM((kv_local, rows, HD), f32),
            pltpu.VMEM((batch_size, positions, heads_local * HD), bf16),
            pair, pair, far, far,
            pltpu.VMEM((steps, STEP_ROWS, width), f32),
            pltpu.VMEM((batch_size, positions, width), bf16),
            dma((3,)),
            dma((reached,)),
            dma((reached, max(columns - 1, 1))),
            dma((batch_size,)),
            dma((reached, PIECES)),
            dma((reached, max(columns - 1, 1))),
            dma((steps,)), dma((2 * (positions // STEP_ROWS),)),
            dma((chips - 1, steps)), dma((chips - 1, steps)),
        ],
        compiler_params=pltpu.CompilerParams(
            collective_id=collective_id, has_side_effects=True, vmem_limit_bytes=56 * 2**20
        ),
    )(slot, x, key_value_weight, query_weight, out_weight, chosen)


def prepare_kernel(
    short, whole, columns, length_hbm, x_hbm, wk_hbm, wv_hbm,
    slot_ref, x_ref, wkv_ref, length_ref, load_sem,
):
    batch_size, positions, _ = x_ref.shape
    half = wkv_ref.shape[1] // 2
    first = lax.axis_index("kv") // columns * columns
    loads = [
        pltpu.make_async_copy(length_hbm, length_ref, load_sem.at[0]),
        pltpu.make_async_copy(wk_hbm, wkv_ref.at[:, pl.ds(0, half)], load_sem.at[1]),
        pltpu.make_async_copy(wv_hbm, wkv_ref.at[:, pl.ds(half, half)], load_sem.at[2]),
    ]
    for load in loads:
        load.start()
    loads[0].wait()

    lengths = [length_ref[b] for b in range(batch_size)]
    ranks = []
    for b in range(batch_size):
        ahead = [
            (lengths[o] >= lengths[b] if o < b else lengths[o] > lengths[b]).astype(jnp.int32)
            for o in range(batch_size) if o != b
        ]
        ranks.append(sum(ahead))
    slots = range(batch_size)
    held = [sum([jnp.where(ranks[b] == j, b, 0) for b in slots]) for j in slots]
    spans = [sum([jnp.where(ranks[b] == j, lengths[b], 0) for b in slots]) for j in slots]
    fits = jnp.int32(1)
    for j in slots:
        fits = fits * (spans[j] <= short[j] * positions).astype(jnp.int32)

    def x_load(j):
        return pltpu.make_async_copy(x_hbm.at[held[j]], x_ref.at[j], load_sem.at[3 + j])

    used = [first < jnp.where(fits > 0, short[j], whole[j]) for j in slots]
    for j in slots:
        @pl.when(used[j])
        def _():
            x_load(j).start()

    slot_ref[0] = fits
    for j in slots:
        slot_ref[1 + j] = held[j]
        slot_ref[1 + batch_size + j] = ranks[j]
        slot_ref[1 + 2 * batch_size + j] = spans[j]
    loads[1].wait()
    loads[2].wait()
    for j in slots:
        @pl.when(used[j])
        def _():
            x_load(j).wait()


def shards(inputs, query_weight, key_weight, value_weight, out_weight, chosen, lengths):
    batch_size, positions, model_width = inputs.shape
    devices = lax.axis_size("kv")
    short, whole = spans(batch_size, devices, positions)
    hbm = pl.BlockSpec(memory_space=pl.ANY)
    vmem = pl.BlockSpec(memory_space=pltpu.VMEM)
    smem = pl.BlockSpec(memory_space=pltpu.SMEM)
    slot, x, key_value_weight = pl.pallas_call(
        functools.partial(prepare_kernel, short, whole, columns_of(devices)),
        out_shape=(
            pltpu.SMEM((1 + 3 * batch_size,), jnp.int32),
            pltpu.VMEM(inputs.shape, inputs.dtype),
            pltpu.VMEM((model_width, 2 * key_weight.shape[1]), key_weight.dtype),
        ),
        in_specs=[hbm] * 4,
        out_specs=(smem, vmem, vmem),
        scratch_shapes=[
            pltpu.SMEM(lengths.shape, jnp.int32),
            pltpu.SemaphoreType.DMA((3 + batch_size,)),
        ],
        compiler_params=pltpu.CompilerParams(vmem_limit_bytes=57 * 2**20),
    )(lengths, inputs, key_weight, value_weight)
    return lax.cond(
        slot[0] > 0,
        functools.partial(layer, short, 0),
        functools.partial(layer, whole, 1),
        slot, x, key_value_weight, query_weight, out_weight, chosen,
    )


def solution(mesh):
    placed = (
        P(None, "kv", None),
        P(None, "tp"),
        P(None, "tp"),
        P(None, "tp"),
        P("tp", None),
        P(None, "kv", None),
        P(),
    )
    return jax.shard_map(
        shards, mesh=mesh, in_specs=placed, out_specs=P(None, "kv", "tp"), check_vma=False
    )
```
